32 devices in a mesh: sp: 16 (over z, y, x), tp: 2 (over core).
Axes of the slice: x: 2, y: 2, z: 4, core: 2. Of those that a mesh axis runs over, the one named last changes fastest.
Arguments:
- tokens: bfloat16 [8192, 3072], P('sp'), may hold values from -72 to 72
- w_query: bfloat16 [3072, 1024], P('sp', 'tp'), may hold values from -0.109375 to 0.109375
- w_key: bfloat16 [3072, 1024], P('sp', 'tp'), may hold values from -0.109375 to 0.109375
- w_value: bfloat16 [3072, 1024], P('sp', 'tp'), may hold values from -0.4375 to 0.4375
- w_out: bfloat16 [1024, 3072], P('tp', 'sp'), may hold values from -0.1875 to 0.1875
Outputs:
- mixed: bfloat16 [8192, 3072], P(('sp', 'tp'))
- row_lse: float32 [16, 8192], P('tp', 'sp')
The draws below stay inside these ranges and needn't reach their ends.
All inputs are finite; a program needn't handle non-finite values.
Results may differ from the reference program's by a relative error of at most 0.014.
Values may be sent and summed in bfloat16 or wider, within the bound.
A program may use at most 64 MiB of HBM per device.

```python
import jax
import jax.numpy as jnp
from jax import lax

D = 3072
HEADS = 16
HEAD_SIZE = 64
KEYS_BEHIND = 128
D_ATT = 1024
SEQUENCE_TOKENS = 8192
N_TP = 2


def draw_tokens(key, part):
    base_offset = jax.random.truncated_normal(key, -6.0, 6.0, (SEQUENCE_TOKENS, D), jnp.float32)
    return base_offset.astype(jnp.bfloat16)


def block_levels(own_key, extent, pieces, least, high):
    factor_of = 1.0
    for dim, blocks in pieces:
        steps = jax.random.uniform(jax.random.fold_in(jax.random.fold_in(own_key, 6), dim), (blocks,), jnp.float32, least / len(pieces), high / len(pieces))
        factor_of = factor_of * jnp.repeat(jnp.exp(steps), extent[dim] // blocks).reshape((-1,) + (1,) * (len(extent) - 1 - dim))
    return factor_of


def centred(key, extent, spread, bound, pieces=(), held_as=jnp.bfloat16):
    result = jax.random.normal(key, extent, jnp.float32) * spread
    if len(pieces) > 0:
        result = block_levels(key, extent, pieces, -0.22, 0.18) * result
    return jnp.clip(result, min=-bound, max=bound).astype(held_as)


def setup_inputs(seed: int = 0) -> dict:
    arg_keys = jax.random.split(jax.random.key(seed), 6)
    tokens = draw_tokens(jax.random.fold_in(arg_keys[5], 71), 0)
    w_query = centred(arg_keys[1], (D, D_ATT), D ** -0.5, 0.109375, ((0, 16), (1, 2)))
    w_key = centred(arg_keys[2], (D, D_ATT), D ** -0.5, 0.109375, ((0, 16), (1, 2)))
    w_value = centred(arg_keys[3], (D, D_ATT), (D // 16) ** -0.5, 0.4375, ((0, 16), (1, 2)))
    w_out = centred(arg_keys[4], (D_ATT, D), D_ATT ** -0.5, 0.1875, ((0, 2), (1, 16)))
    return {"tokens": tokens, "w_query": w_query, "w_key": w_key, "w_value": w_value, "w_out": w_out}


dilation_rates = (1, 4, 16)
neg_big = -1e30


def band(query_class_rows, key_class_rows, value_class_rows, key_first_index):
    sequence_length = query_class_rows.shape[0]
    if sequence_length <= KEYS_BEHIND:
        blocks = 1
        step = sequence_length
        q_blk = query_class_rows[None]
        k_blk = key_class_rows[None]
        v_blk = value_class_rows[None]
    else:
        blocks = sequence_length // KEYS_BEHIND
        step = KEYS_BEHIND
        q_blk = query_class_rows.reshape(blocks, KEYS_BEHIND, HEAD_SIZE)
        k_rows = key_class_rows.reshape(blocks + 1, KEYS_BEHIND, HEAD_SIZE)
        v_rows = value_class_rows.reshape(blocks + 1, KEYS_BEHIND, HEAD_SIZE)
        k_blk = jnp.concatenate([k_rows[:-1], k_rows[1:]], axis=1)
        v_blk = jnp.concatenate([v_rows[:-1], v_rows[1:]], axis=1)
    score = jnp.einsum('nqd,nkd->nqk', q_blk.astype(jnp.float32), k_blk.astype(jnp.float32)) * (HEAD_SIZE ** -0.5)
    row_at = jnp.arange(step, dtype=jnp.int32)[:, None]
    col_at = jnp.arange(k_blk.shape[1], dtype=jnp.int32)[None, :]
    dist = KEYS_BEHIND + row_at - col_at
    key_pos = key_first_index + jnp.arange(blocks, dtype=jnp.int32)[:, None, None] * step + col_at[None]
    mask = (dist >= 0) & (dist <= KEYS_BEHIND) & (key_pos >= 0)
    score = jnp.where(mask, score, neg_big)
    top = jnp.max(score, axis=-1, keepdims=True)
    weight = jnp.exp(score - top)
    denom = jnp.sum(weight, axis=-1)
    weight_bf = weight.astype(jnp.bfloat16)
    out = jnp.einsum('nqk,nkd->nqd', weight_bf.astype(jnp.float32), v_blk.astype(jnp.float32)) / denom[..., None]
    lse = top[..., 0] + jnp.log(denom)
    return out.reshape(sequence_length, HEAD_SIZE), lse.reshape(sequence_length)


def one_head(parts):
    query_head_rows, key_head_rows, value_head_rows = parts
    outs = []
    lses = []
    for dilation_rate in dilation_rates:
        sequence_length = SEQUENCE_TOKENS // dilation_rate
        query_class_rows = query_head_rows.reshape(sequence_length, dilation_rate, HEAD_SIZE).transpose(1, 0, 2)
        padding_rows = jnp.zeros((KEYS_BEHIND * dilation_rate, HEAD_SIZE), jnp.bfloat16)
        key_class_rows = jnp.concatenate([padding_rows, key_head_rows], 0).reshape(KEYS_BEHIND + sequence_length, dilation_rate, HEAD_SIZE).transpose(1, 0, 2)
        value_class_rows = jnp.concatenate([padding_rows, value_head_rows], 0).reshape(KEYS_BEHIND + sequence_length, dilation_rate, HEAD_SIZE).transpose(1, 0, 2)
        out, lse = jax.vmap(lambda a, b, c: band(a, b, c, -KEYS_BEHIND))(query_class_rows, key_class_rows, value_class_rows)
        outs.append(out.transpose(1, 0, 2).reshape(SEQUENCE_TOKENS, HEAD_SIZE))
        lses.append(lse.T.reshape(SEQUENCE_TOKENS))
    lse_all = jnp.stack(lses, 0)
    peak = jnp.max(lse_all, axis=0)
    expo = jnp.exp(lse_all - peak)
    total = jnp.sum(expo, axis=0)
    mix = expo / total
    attended = jnp.sum(mix[..., None] * jnp.stack(outs, 0), axis=0)
    return attended, peak + jnp.log(total)


def reference(tokens, w_query, w_key, w_value, w_out):
    query_input = jnp.dot(tokens, w_query, preferred_element_type=jnp.float32).astype(jnp.bfloat16)
    keys = jnp.dot(tokens, w_key, preferred_element_type=jnp.float32).astype(jnp.bfloat16)
    values = jnp.dot(tokens, w_value, preferred_element_type=jnp.float32).astype(jnp.bfloat16)

    def heads_first(a):
        return a.reshape(SEQUENCE_TOKENS, HEADS, HEAD_SIZE).transpose(1, 0, 2)

    attended, row_lse = lax.map(one_head, (heads_first(query_input), heads_first(keys), heads_first(values)))
    attended = attended.transpose(1, 0, 2).reshape(SEQUENCE_TOKENS, D_ATT).astype(jnp.bfloat16)
    cols = D_ATT // N_TP
    total = jnp.zeros((SEQUENCE_TOKENS, D), jnp.float32)
    for group in range(N_TP):
        part = jnp.dot(attended[:, group * cols:(group + 1) * cols], w_out[group * cols:(group + 1) * cols],
                       preferred_element_type=jnp.float32).astype(jnp.bfloat16)
        total = total + part.astype(jnp.float32)
    return total.astype(jnp.bfloat16), row_lse
```

```python
import functools

import jax
import jax.numpy as jnp
from jax import lax
from jax.experimental import pallas as pl
from jax.experimental.pallas import tpu as pltpu
from jax.sharding import PartitionSpec as P

HEAD_SIZE = 64
KEYS_BEHIND = 128
LANES = 128

dilation_rates = (1, 4, 16)
neg_big = -1e30

MESH = pl.DeviceIdType.MESH
VMEM = pltpu.VMEM


def at(sp, tp):
    return {"sp": sp, "tp": tp}


def project_kernel(
    n, n_tp, group, far, w_ref, tok_ref, q_ref, kv_ref, halo_ref,
    tok_all, w_all, w1_send, w1_recv, w2_send, w2_recv,
    t_send, t_recv, d_send, d_recv, f_send, f_recv, h_send, h_recv, own_sem,
):
    sp, tp = lax.axis_index("sp"), lax.axis_index("tp")
    planes = n // group
    g, plane = lax.rem(sp, group), sp // group
    rows = tok_ref.shape[0]
    part = rows // n_tp
    half = part // 2

    barrier = pltpu.get_barrier_semaphore()

    def greet(j, _):
        pl.semaphore_signal(barrier, inc=1, device_id=at(lax.rem(sp + j, n), tp), device_id_type=MESH)
        return _

    lax.fori_loop(1, n, greet, 0)
    for j in range(1, n_tp):
        pl.semaphore_signal(barrier, inc=1, device_id=at(sp, lax.rem(tp + j, n_tp)), device_id_type=MESH)

    own_t = pltpu.make_async_copy(tok_ref, tok_all.at[g], own_sem.at[0])
    own_w = pltpu.make_async_copy(w_ref.at[g], w_all.at[sp], own_sem.at[1])
    own_t.start()
    own_w.start()
    pl.semaphore_wait(barrier, n - 1 + n_tp - 1)

    def mate(i):
        return plane * group + (g ^ i)

    def w_in_plane(i):
        return pltpu.make_async_remote_copy(
            src_ref=w_ref.at[g ^ i], dst_ref=w_all.at[sp], send_sem=w1_send.at[i], recv_sem=w1_recv.at[i],
            device_id=at(mate(i), tp), device_id_type=MESH)

    def w_in_plane_arrives(i):
        return pltpu.make_async_remote_copy(
            src_ref=w_ref.at[g ^ i], dst_ref=w_all.at[mate(i)], send_sem=w1_send.at[i], recv_sem=w1_recv.at[i],
            device_id=at(mate(i), tp), device_id_type=MESH)

    def w_to_plane(i, k):
        source = w_ref.at[g] if i == 0 else w_all.at[mate(i)]
        return pltpu.make_async_remote_copy(
            src_ref=source, dst_ref=w_all.at[mate(i)],
            send_sem=w2_send.at[i, k], recv_sem=w2_recv.at[i, k],
            device_id=at(lax.rem(sp + k * group, n), tp), device_id_type=MESH)

    def w_to_plane_arrives(i, k):
        origin = lax.rem(plane + planes - k, planes) * group + (g ^ i)
        return pltpu.make_async_remote_copy(
            src_ref=w_ref.at[g], dst_ref=w_all.at[origin],
            send_sem=w2_send.at[i, k], recv_sem=w2_recv.at[i, k],
            device_id=at(lax.rem(sp + k * group, n), tp), device_id_type=MESH)

    mine = pl.ds(pl.multiple_of(tp * part, part), part)

    def halves(k):
        return pl.ds(pl.multiple_of(tp * part + k * half, half), half)

    def tokens_out(i):
        return pltpu.make_async_remote_copy(
            src_ref=tok_ref.at[mine], dst_ref=tok_all.at[g, mine], send_sem=t_send.at[i], recv_sem=t_recv.at[i],
            device_id=at(mate(i), tp), device_id_type=MESH)

    def tokens_in(i):
        return pltpu.make_async_remote_copy(
            src_ref=tok_ref.at[mine], dst_ref=tok_all.at[g ^ i, mine], send_sem=t_send.at[i], recv_sem=t_recv.at[i],
            device_id=at(mate(i), tp), device_id_type=MESH)

    def corner_out(i):
        ref = tok_all.at[g ^ i, halves(i - 1)]
        return pltpu.make_async_remote_copy(
            src_ref=ref, dst_ref=ref, send_sem=d_send.at[i], recv_sem=d_recv.at[i],
            device_id=at(mate(3 - i), tp), device_id_type=MESH)

    def corner_in(i):
        ref = tok_all.at[g ^ 3, halves(i - 1)]
        return pltpu.make_async_remote_copy(
            src_ref=ref, dst_ref=ref, send_sem=d_send.at[i], recv_sem=d_recv.at[i],
            device_id=at(mate(3 - i), tp), device_id_type=MESH)

    def across(i, j):
        ref = tok_all.at[g ^ i, mine]
        return pltpu.make_async_remote_copy(
            src_ref=ref, dst_ref=ref, send_sem=f_send.at[i, j], recv_sem=f_recv.at[i, j],
            device_id=at(sp, lax.rem(tp + j, n_tp)), device_id_type=MESH)

    def across_in(i, j):
        origin = lax.rem(tp + n_tp - j, n_tp)
        ref = tok_all.at[g ^ i, pl.ds(pl.multiple_of(origin * part, part), part)]
        return pltpu.make_async_remote_copy(
            src_ref=ref, dst_ref=ref, send_sem=f_send.at[i, j], recv_sem=f_recv.at[i, j],
            device_id=at(sp, lax.rem(tp + j, n_tp)), device_id_type=MESH)

    near = [i for i in (1, 2) if i < group]
    for i in range(1, group):
        w_in_plane(i).start()
    if planes > 1:
        lax.fori_loop(1, planes, lambda k, _: (w_to_plane(0, k).start(), _)[1], 0)
    for i in near:
        tokens_out(i).start()
    for i in range(1, group):
        w_in_plane_arrives(i).wait_recv()
        if planes > 1:
            lax.fori_loop(1, planes, lambda k, _, i=i: (w_to_plane(i, k).start(), _)[1], 0)
    for i in near:
        tokens_in(i).wait_recv()
        if group == 4:
            corner_out(i).start()
        for j in range(1, n_tp):
            across(i, j).start()

    own_w.wait()
    own_t.wait()
    for i in range(group):
        if planes > 1:
            lax.fori_loop(1, planes, lambda k, _, i=i: (w_to_plane_arrives(i, k).wait_recv(), _)[1], 0)

    def halo_block(h, b):
        view = pl.ds(pl.multiple_of(b * rows, rows), rows)
        return view

    def halo_out(h, i):
        view = pl.ds(pl.multiple_of((g ^ i) * rows, rows), rows)
        return pltpu.make_async_remote_copy(
            src_ref=kv_ref.at[view], dst_ref=halo_ref.at[far - h, view],
            send_sem=h_send.at[h, i], recv_sem=h_recv.at[h, i],
            device_id=at(lax.rem(sp + h * group, n), tp), device_id_type=MESH)

    tile = min(256, rows)

    for i in range(group):
        if i == 3:
            for k in (1, 2):
                corner_in(k).wait_recv()
            for j in range(1, n_tp):
                across(i, j).start()
        if i > 0:
            for j in range(1, n_tp):
                across_in(i, j).wait_recv()
        block = g ^ i

        def one(s, _, block=block):
            x = tok_all[block, pl.ds(pl.multiple_of(s * tile, tile), tile), :]
            w = w_all[...].reshape(-1, 3 * LANES)
            y = jnp.dot(x, w, preferred_element_type=jnp.float32).astype(jnp.bfloat16)
            to = pl.ds(pl.multiple_of(block * rows + s * tile, tile), tile)
            q_ref[to, :] = y[:, :LANES]
            kv_ref[to, :] = y[:, LANES:]
            return _

        lax.fori_loop(0, rows // tile, one, 0)
        for h in range(1, far + 1):
            @pl.when(plane + h < planes)
            def _():
                halo_out(h, i).start()

    for h in range(1, far + 1):
        @pl.when(plane - h >= 0)
        def _():
            for i in range(group):
                halo_out(h, i).wait_recv()

        @pl.when(plane - h < 0)
        def _():
            halo_ref[far - h] = jnp.zeros(halo_ref.shape[1:], halo_ref.dtype)

        @pl.when(plane + h < planes)
        def _():
            for i in range(group):
                halo_out(h, i).wait_send()

    for i in range(1, group):
        w_in_plane(i).wait_send()
        for j in range(1, n_tp):
            across(i, j).wait_send()
    for i in near:
        tokens_out(i).wait_send()
        if group == 4:
            corner_out(i).wait_send()
    if planes > 1:
        for i in range(group):
            lax.fori_loop(1, planes, lambda k, _, i=i: (w_to_plane(i, k).wait_send(), _)[1], 0)


def attend_kernel(heads, base_ref, q_ref, kv_ref, halo_ref, att_ref, lse_ref, qs, ks, vs, top_s, den_s, acc_s):
    base = base_ref[0]
    own = q_ref.shape[0]
    behind = ks.shape[0] - own
    pieces, piece_rows = halo_ref.shape[0], halo_ref.shape[1]
    qs[...] = q_ref[...].astype(jnp.float32) * HEAD_SIZE ** (-0.5)
    for h in range(pieces):
        ks[h * piece_rows : (h + 1) * piece_rows] = halo_ref[h, :, :LANES].astype(jnp.float32)
        vs[h * piece_rows : (h + 1) * piece_rows] = halo_ref[h, :, LANES:].astype(jnp.float32)
    ks[behind:] = kv_ref[:, :LANES].astype(jnp.float32)
    vs[behind:] = kv_ref[:, LANES:].astype(jnp.float32)

    for number, d in enumerate(dilation_rates):
        step = min(KEYS_BEHIND, own // d)
        count = own // d // step
        span = step + KEYS_BEHIND

        def block(index, _, number=number, d=d, step=step, span=span):
            cls, b = lax.rem(index, d), index // d
            start = b * (step * d) + cls
            q_at = pl.ds(start, step, stride=d) if d > 1 else pl.ds(pl.multiple_of(start, step), step)
            k_start = behind - KEYS_BEHIND * d + start
            k_at = pl.ds(k_start, span, stride=d) if d > 1 else pl.ds(pl.multiple_of(k_start, step), span)
            q = qs[q_at, :]
            k = ks[k_at, :].astype(jnp.bfloat16)
            v = vs[k_at, :].astype(jnp.bfloat16)
            low = lax.broadcasted_iota(jnp.int32, (step, LANES), 1) < HEAD_SIZE
            q2 = jnp.concatenate([jnp.where(low, q, 0.0), jnp.where(low, 0.0, q)], axis=0).astype(jnp.bfloat16)
            s = lax.dot_general(q2, k, (((1,), (1,)), ((), ())), preferred_element_type=jnp.float32)
            row = lax.broadcasted_iota(jnp.int32, (step, span), 0)
            col = lax.broadcasted_iota(jnp.int32, (step, span), 1)
            dist = KEYS_BEHIND + row - col
            first = base // d + b * step - KEYS_BEHIND
            seen = (dist >= 0) & (dist <= KEYS_BEHIND) & (first + col >= 0)
            s = jnp.where(jnp.concatenate([seen, seen], axis=0), s, neg_big)
            top = jnp.max(s, axis=1, keepdims=True)
            p = jnp.exp(s - top)
            den = jnp.sum(p, axis=1, keepdims=True)
            o = jnp.dot(p.astype(jnp.bfloat16), v, preferred_element_type=jnp.float32)
            top = jnp.where(low, top[:step], top[step:])
            den = jnp.where(low, den[:step], den[step:])
            o = jnp.where(low, o[:step], o[step:])
            if number == 0:
                top_s[q_at, :] = top
                den_s[q_at, :] = den
                acc_s[q_at, :] = o
            else:
                was = top_s[q_at, :]
                new = jnp.maximum(was, top)
                old_scale, scale = jnp.exp(was - new), jnp.exp(top - new)
                top_s[q_at, :] = new
                den_s[q_at, :] = den_s[q_at, :] * old_scale + den * scale
                acc_s[q_at, :] = acc_s[q_at, :] * old_scale + o * scale
            return _

        lax.fori_loop(0, d * count, block, 0, unroll=2)

    rows = lse_ref.shape[2]
    att_ref[...] = (acc_s[...] / den_s[...]).astype(jnp.bfloat16)
    for t in range(own // LANES):
        at_rows = pl.ds(t * LANES, LANES)
        lse = (top_s[at_rows, :] + jnp.log(den_s[at_rows, :])).T
        b, off = (t * LANES) // rows, (t * LANES) % rows
        for h in range(heads):
            lse_ref[b, h : h + 1, off : off + LANES] = lse[h * HEAD_SIZE : h * HEAD_SIZE + 1, :]


def return_kernel(n_tp, group, att_ref, lse_ref, all_ref, lse_all, a_send, a_recv, l_send, l_recv, own_sem):
    sp, tp = lax.axis_index("sp"), lax.axis_index("tp")
    g, plane = lax.rem(sp, group), sp // group
    part = all_ref.shape[0]
    width = all_ref.shape[1] // n_tp
    others = [(i, j) for i in range(group) for j in range(n_tp) if (i, j) != (0, 0)]

    def device(i, j):
        return plane * group + (g ^ i), lax.rem(tp + j, n_tp)

    barrier = pltpu.get_barrier_semaphore()
    for i, j in others:
        pl.semaphore_signal(barrier, inc=1, device_id=at(*device(i, j)), device_id_type=MESH)

    def columns(h, c):
        return pl.ds(pl.multiple_of(c * width + h * LANES, LANES), LANES)

    def sent_rows(i, j):
        c = lax.rem(tp + j, n_tp)
        return pl.ds(pl.multiple_of((g ^ i) * (part * n_tp) + c * part, part), part)

    own = pltpu.make_async_copy(att_ref.at[sent_rows(0, 0)], all_ref.at[:, columns(g, tp)], own_sem.at[0])
    own_l = pltpu.make_async_copy(lse_ref.at[g], lse_all.at[g], own_sem.at[1])
    own.start()
    own_l.start()
    pl.semaphore_wait(barrier, len(others))

    def out(i, j):
        return pltpu.make_async_remote_copy(
            src_ref=att_ref.at[sent_rows(i, j)], dst_ref=all_ref.at[:, columns(g, tp)],
            send_sem=a_send.at[i, j], recv_sem=a_recv.at[i, j], device_id=at(*device(i, j)), device_id_type=MESH)

    def arrives(i, j):
        return pltpu.make_async_remote_copy(
            src_ref=att_ref.at[sent_rows(i, j)],
            dst_ref=all_ref.at[:, columns(g ^ i, lax.rem(tp + n_tp - j, n_tp))],
            send_sem=a_send.at[i, j], recv_sem=a_recv.at[i, j], device_id=at(*device(i, j)), device_id_type=MESH)

    def lse_out(i):
        return pltpu.make_async_remote_copy(
            src_ref=lse_ref.at[g ^ i], dst_ref=lse_all.at[g], send_sem=l_send.at[i], recv_sem=l_recv.at[i],
            device_id=at(*device(i, 0)), device_id_type=MESH)

    def lse_in(i):
        return pltpu.make_async_remote_copy(
            src_ref=lse_ref.at[g ^ i], dst_ref=lse_all.at[g ^ i], send_sem=l_send.at[i], recv_sem=l_recv.at[i],
            device_id=at(*device(i, 0)), device_id_type=MESH)

    for i, j in others:
        out(i, j).start()
    for i in range(1, group):
        lse_out(i).start()
    own.wait()
    own_l.wait()
    for i, j in others:
        arrives(i, j).wait_recv()
    for i in range(1, group):
        lse_in(i).wait_recv()
    for i, j in others:
        out(i, j).wait_send()
    for i in range(1, group):
        lse_out(i).wait_send()


def shards(n, n_tp, tokens, w_query, w_key, w_value, w_out):
    rows, model = tokens.shape
    depth, width = w_query.shape
    slabs = width // LANES
    reach = KEYS_BEHIND * dilation_rates[-1]
    group = 1
    while group < 4 and group * rows < reach and slabs % (2 * group) == 0 and n % (2 * group) == 0:
        group *= 2
    assert slabs == group
    far = (reach + group * rows - 1) // (group * rows)
    planes = n // group
    own = group * rows
    part = rows // n_tp
    heads = LANES // HEAD_SIZE

    full_out = lax.all_gather(w_out, "sp", axis=1, tiled=True)
    full_out = lax.all_gather(full_out, "tp", axis=0, tiled=True)

    w = jnp.stack([w_query, w_key, w_value], 1).reshape(depth, 3, group, LANES)
    w = w.transpose(2, 0, 1, 3).reshape(group, depth, 3 * LANES)

    dma = pltpu.SemaphoreType.DMA
    vmem = pl.BlockSpec(memory_space=VMEM)
    q, kv, halo = pl.pallas_call(
        functools.partial(project_kernel, n, n_tp, group, far),
        out_shape=(
            jax.ShapeDtypeStruct((own, LANES), jnp.bfloat16),
            jax.ShapeDtypeStruct((own, 2 * LANES), jnp.bfloat16),
            jax.ShapeDtypeStruct((far, own, 2 * LANES), jnp.bfloat16),
        ),
        in_specs=[vmem, pl.BlockSpec(memory_space=pl.ANY)],
        out_specs=(vmem, vmem, vmem),
        scratch_shapes=[
            VMEM((group, rows, model), jnp.bfloat16),
            VMEM((n, depth, 3 * LANES), jnp.bfloat16),
            dma((group,)), dma((group,)),
            dma((group, planes)), dma((group, planes)),
            dma((group,)), dma((group,)),
            dma((group,)), dma((group,)),
            dma((group, n_tp)), dma((group, n_tp)),
            dma((far + 1, group)), dma((far + 1, group)),
            dma((2,)),
        ],
        compiler_params=pltpu.CompilerParams(collective_id=0, has_side_effects=True, vmem_limit_bytes=48 << 20),
        cost_estimate=pl.CostEstimate(flops=2 * own * model * 3 * LANES, bytes_accessed=1 << 24, transcendentals=0),
        name="project",
    )(w, tokens)

    base = (lax.axis_index("sp") // group * own).astype(jnp.int32).reshape(1)
    behind = far * own
    f32 = jnp.float32
    att, lse = pl.pallas_call(
        functools.partial(attend_kernel, heads),
        out_shape=(
            jax.ShapeDtypeStruct((own, LANES), jnp.bfloat16),
            jax.ShapeDtypeStruct((group, heads, rows), f32),
        ),
        in_specs=[pl.BlockSpec(memory_space=pltpu.SMEM), vmem, vmem, vmem],
        out_specs=(vmem, vmem),
        scratch_shapes=[
            VMEM((own, LANES), f32), VMEM((behind + own, LANES), f32), VMEM((behind + own, LANES), f32),
            VMEM((own, LANES), f32), VMEM((own, LANES), f32), VMEM((own, LANES), f32),
        ],
        compiler_params=pltpu.CompilerParams(vmem_limit_bytes=32 << 20),
        cost_estimate=pl.CostEstimate(flops=1 << 32, bytes_accessed=1 << 22, transcendentals=1 << 22),
        name="attend",
    )(base, q, kv, halo)

    attended, lse_all = pl.pallas_call(
        functools.partial(return_kernel, n_tp, group),
        out_shape=(
            jax.ShapeDtypeStruct((part, n_tp * width), jnp.bfloat16),
            jax.ShapeDtypeStruct((group, heads, rows), f32),
        ),
        in_specs=[vmem, vmem],
        out_specs=(vmem, vmem),
        scratch_shapes=[
            dma((group, n_tp)), dma((group, n_tp)), dma((group,)), dma((group,)), dma((2,)),
        ],
        compiler_params=pltpu.CompilerParams(collective_id=1, has_side_effects=True),
        name="hand_back",
    )(att, lse)

    mixed = jnp.dot(attended, full_out, preferred_element_type=f32).astype(jnp.bfloat16)
    return mixed, lse_all.reshape(group * heads, rows)


def solution(mesh):
    placed = (P("sp", None), P("sp", "tp"), P("sp", "tp"), P("sp", "tp"), P("tp", "sp"))
    return jax.shard_map(
        functools.partial(shards, mesh.shape["sp"], mesh.shape["tp"]),
        mesh=mesh,
        in_specs=placed,
        out_specs=(P(("sp", "tp"), None), P("tp", "sp")),
        check_vma=False,
    )
```

```python
import functools

import jax
import jax.numpy as jnp
from jax import lax
from jax.experimental import pallas as pl
from jax.experimental.pallas import tpu as pltpu
from jax.sharding import PartitionSpec as P

HEAD_SIZE = 64
KEYS_BEHIND = 128
LANES = 128

dilation_rates = (1, 4, 16)
neg_big = -1e30

MESH = pl.DeviceIdType.MESH
VMEM = pltpu.VMEM


def at(sp, tp):
    return {"sp": sp, "tp": tp}


def project_kernel(
    n, n_tp, group, far, w_ref, tok_ref, q_ref, kv_ref, halo_ref,
    tok_all, w_all, w1_send, w1_recv, w2_send, w2_recv,
    t_send, t_recv, d_send, d_recv, f_send, f_recv, h_send, h_recv, own_sem,
):
    sp, tp = lax.axis_index("sp"), lax.axis_index("tp")
    planes = n // group
    g, plane = lax.rem(sp, group), sp // group
    rows = tok_ref.shape[0]
    part = rows // n_tp
    half = part // 2

    barrier = pltpu.get_barrier_semaphore()

    def greet(j, _):
        pl.semaphore_signal(barrier, inc=1, device_id=at(lax.rem(sp + j, n), tp), device_id_type=MESH)
        return _

    lax.fori_loop(1, n, greet, 0)
    for j in range(1, n_tp):
        pl.semaphore_signal(barrier, inc=1, device_id=at(sp, lax.rem(tp + j, n_tp)), device_id_type=MESH)

    own_t = pltpu.make_async_copy(tok_ref, tok_all.at[g], own_sem.at[0])
    own_w = pltpu.make_async_copy(w_ref.at[g], w_all.at[sp], own_sem.at[1])
    own_t.start()
    own_w.start()
    pl.semaphore_wait(barrier, n - 1 + n_tp - 1)

    def mate(i):
        return plane * group + (g ^ i)

    def w_in_plane(i):
        return pltpu.make_async_remote_copy(
            src_ref=w_ref.at[g ^ i], dst_ref=w_all.at[sp], send_sem=w1_send.at[i], recv_sem=w1_recv.at[i],
            device_id=at(mate(i), tp), device_id_type=MESH)

    def w_in_plane_arrives(i):
        return pltpu.make_async_remote_copy(
            src_ref=w_ref.at[g ^ i], dst_ref=w_all.at[mate(i)], send_sem=w1_send.at[i], recv_sem=w1_recv.at[i],
            device_id=at(mate(i), tp), device_id_type=MESH)

    def w_to_plane(i, k):
        source = w_ref.at[g] if i == 0 else w_all.at[mate(i)]
        return pltpu.make_async_remote_copy(
            src_ref=source, dst_ref=w_all.at[mate(i)],
            send_sem=w2_send.at[i, k], recv_sem=w2_recv.at[i, k],
            device_id=at(lax.rem(sp + k * group, n), tp), device_id_type=MESH)

    def w_to_plane_arrives(i, k):
        origin = lax.rem(plane + planes - k, planes) * group + (g ^ i)
        return pltpu.make_async_remote_copy(
            src_ref=w_ref.at[g], dst_ref=w_all.at[origin],
            send_sem=w2_send.at[i, k], recv_sem=w2_recv.at[i, k],
            device_id=at(lax.rem(sp + k * group, n), tp), device_id_type=MESH)

    mine = pl.ds(pl.multiple_of(tp * part, part), part)

    def halves(k):
        return pl.ds(pl.multiple_of(tp * part + k * half, half), half)

    def tokens_out(i):
        return pltpu.make_async_remote_copy(
            src_ref=tok_ref.at[mine], dst_ref=tok_all.at[g, mine], send_sem=t_send.at[i], recv_sem=t_recv.at[i],
            device_id=at(mate(i), tp), device_id_type=MESH)

    def tokens_in(i):
        return pltpu.make_async_remote_copy(
            src_ref=tok_ref.at[mine], dst_ref=tok_all.at[g ^ i, mine], send_sem=t_send.at[i], recv_sem=t_recv.at[i],
            device_id=at(mate(i), tp), device_id_type=MESH)

    def corner_out(i):
        ref = tok_all.at[g ^ i, halves(i - 1)]
        return pltpu.make_async_remote_copy(
            src_ref=ref, dst_ref=ref, send_sem=d_send.at[i], recv_sem=d_recv.at[i],
            device_id=at(mate(3 - i), tp), device_id_type=MESH)

    def corner_in(i):
        ref = tok_all.at[g ^ 3, halves(i - 1)]
        return pltpu.make_async_remote_copy(
            src_ref=ref, dst_ref=ref, send_sem=d_send.at[i], recv_sem=d_recv.at[i],
            device_id=at(mate(3 - i), tp), device_id_type=MESH)

    def across(i, j):
        ref = tok_all.at[g ^ i, mine]
        return pltpu.make_async_remote_copy(
            src_ref=ref, dst_ref=ref, send_sem=f_send.at[i, j], recv_sem=f_recv.at[i, j],
            device_id=at(sp, lax.rem(tp + j, n_tp)), device_id_type=MESH)

    def across_in(i, j):
        origin = lax.rem(tp + n_tp - j, n_tp)
        ref = tok_all.at[g ^ i, pl.ds(pl.multiple_of(origin * part, part), part)]
        return pltpu.make_async_remote_copy(
            src_ref=ref, dst_ref=ref, send_sem=f_send.at[i, j], recv_sem=f_recv.at[i, j],
            device_id=at(sp, lax.rem(tp + j, n_tp)), device_id_type=MESH)

    near = [i for i in (1, 2) if i < group]
    for i in range(1, group):
        w_in_plane(i).start()
    if planes > 1:
        lax.fori_loop(1, planes, lambda k, _: (w_to_plane(0, k).start(), _)[1], 0)
    for i in near:
        tokens_out(i).start()
    for i in range(1, group):
        w_in_plane_arrives(i).wait_recv()
        if planes > 1:
            lax.fori_loop(1, planes, lambda k, _, i=i: (w_to_plane(i, k).start(), _)[1], 0)
    for i in near:
        tokens_in(i).wait_recv()
        if group == 4:
            corner_out(i).start()
        for j in range(1, n_tp):
            across(i, j).start()

    own_w.wait()
    own_t.wait()
    for i in range(group):
        if planes > 1:
            lax.fori_loop(1, planes, lambda k, _, i=i: (w_to_plane_arrives(i, k).wait_recv(), _)[1], 0)

    def halo_block(h, b):
        view = pl.ds(pl.multiple_of(b * rows, rows), rows)
        return view

    def halo_out(h, i):
        view = pl.ds(pl.multiple_of((g ^ i) * rows, rows), rows)
        return pltpu.make_async_remote_copy(
            src_ref=kv_ref.at[view], dst_ref=halo_ref.at[far - h, view],
            send_sem=h_send.at[h, i], recv_sem=h_recv.at[h, i],
            device_id=at(lax.rem(sp + h * group, n), tp), device_id_type=MESH)

    tile = min(256, rows)

    for i in range(group):
        if i == 3:
            for k in (1, 2):
                corner_in(k).wait_recv()
            for j in range(1, n_tp):
                across(i, j).start()
        if i > 0:
            for j in range(1, n_tp):
                across_in(i, j).wait_recv()
        block = g ^ i

        def one(s, _, block=block):
            x = tok_all[block, pl.ds(pl.multiple_of(s * tile, tile), tile), :]
            w = w_all[...].reshape(-1, 3 * LANES)
            y = jnp.dot(x, w, preferred_element_type=jnp.float32).astype(jnp.bfloat16)
            to = pl.ds(pl.multiple_of(block * rows + s * tile, tile), tile)
            q_ref[to, :] = y[:, :LANES]
            kv_ref[to, :] = y[:, LANES:]
            return _

        lax.fori_loop(0, rows // tile, one, 0)
        for h in range(1, far + 1):
            @pl.when(plane + h < planes)
            def _():
                halo_out(h, i).start()

    for h in range(1, far + 1):
        @pl.when(plane - h >= 0)
        def _():
            for i in range(group):
                halo_out(h, i).wait_recv()

        @pl.when(plane - h < 0)
        def _():
            halo_ref[far - h] = jnp.zeros(halo_ref.shape[1:], halo_ref.dtype)

        @pl.when(plane + h < planes)
        def _():
            for i in range(group):
                halo_out(h, i).wait_send()

    for i in range(1, group):
        w_in_plane(i).wait_send()
        for j in range(1, n_tp):
            across(i, j).wait_send()
    for i in near:
        tokens_out(i).wait_send()
        if group == 4:
            corner_out(i).wait_send()
    if planes > 1:
        for i in range(group):
            lax.fori_loop(1, planes, lambda k, _, i=i: (w_to_plane(i, k).wait_send(), _)[1], 0)


def attend_kernel(
    n, n_tp, group, heads, q_ref, kv_ref, halo_ref, o_ref, mixed_ref, lse_all,
    qs, ks, vs, top_s, den_s, acc_s, att, lse_ref, o_all, att_all, sums, sums_in,
    z_send, z_recv, b_send, b_recv, c_send, c_recv, a_send, a_recv, l_send, l_recv, s_send, s_recv, own_sem,
):
    sp, tp = lax.axis_index("sp"), lax.axis_index("tp")
    planes = n // group
    g, plane = lax.rem(sp, group), sp // group
    own = q_ref.shape[0]
    base = plane * own
    rows = lse_all.shape[2]
    part = mixed_ref.shape[0]
    cut, width = o_ref.shape
    half = cut // 2

    def mate(i):
        return plane * group + (g ^ i)

    barrier = pltpu.get_barrier_semaphore()

    def greet(k, _):
        pl.semaphore_signal(barrier, inc=1, device_id=at(lax.rem(sp + k * group, n), tp), device_id_type=MESH)
        return _

    lax.fori_loop(1, planes, greet, 0)
    for i in range(1, group):
        pl.semaphore_signal(barrier, inc=1, device_id=at(mate(i), tp), device_id_type=MESH)
    for j in range(1, n_tp):
        pl.semaphore_signal(barrier, inc=1, device_id=at(sp, lax.rem(tp + j, n_tp)), device_id_type=MESH)

    def strip(k, i, part_of=None):
        origin = lax.rem(plane + planes - k, planes) * group + (g ^ i)
        if part_of is None:
            return o_all.at[pl.ds(pl.multiple_of(origin * cut, cut), cut)]
        return o_all.at[pl.ds(pl.multiple_of(origin * cut + part_of * half, half), half)]

    def z_out(k):
        return pltpu.make_async_remote_copy(
            src_ref=o_ref, dst_ref=strip(0, 0), send_sem=z_send.at[k], recv_sem=z_recv.at[k],
            device_id=at(lax.rem(sp + k * group, n), tp), device_id_type=MESH)

    def z_in(k):
        return pltpu.make_async_remote_copy(
            src_ref=o_ref, dst_ref=strip(k, 0), send_sem=z_send.at[k], recv_sem=z_recv.at[k],
            device_id=at(lax.rem(sp + k * group, n), tp), device_id_type=MESH)

    def side_out(k, i):
        return pltpu.make_async_remote_copy(
            src_ref=strip(k, 0), dst_ref=strip(k, 0), send_sem=b_send.at[k, i], recv_sem=b_recv.at[k, i],
            device_id=at(mate(i), tp), device_id_type=MESH)

    def side_in(k, i):
        return pltpu.make_async_remote_copy(
            src_ref=strip(k, i), dst_ref=strip(k, i), send_sem=b_send.at[k, i], recv_sem=b_recv.at[k, i],
            device_id=at(mate(i), tp), device_id_type=MESH)

    def corner_out(k, i):
        return pltpu.make_async_remote_copy(
            src_ref=strip(k, i, i - 1), dst_ref=strip(k, i, i - 1), send_sem=c_send.at[k, i], recv_sem=c_recv.at[k, i],
            device_id=at(mate(3 - i), tp), device_id_type=MESH)

    def corner_in(k, i):
        return pltpu.make_async_remote_copy(
            src_ref=strip(k, 3, i - 1), dst_ref=strip(k, 3, i - 1), send_sem=c_send.at[k, i], recv_sem=c_recv.at[k, i],
            device_id=at(mate(3 - i), tp), device_id_type=MESH)

    near = [i for i in (1, 2) if i < group]

    def sides(k):
        for i in near:
            side_out(k, i).start()

    def corners(k):
        for i in near:
            side_in(k, i).wait_recv()
            if group == 4:
                corner_out(k, i).start()

    own_o = pltpu.make_async_copy(o_ref, strip(0, 0), own_sem.at[0])
    own_o.start()
    pl.semaphore_wait(barrier, planes - 1 + group - 1 + n_tp - 1)
    if planes > 1:
        lax.fori_loop(1, planes, lambda k, _: (z_out(k).start(), _)[1], 0)
    own_o.wait()
    sides(0)

    behind = ks.shape[0] - own
    pieces, piece_rows = halo_ref.shape[0], halo_ref.shape[1]
    qs[...] = q_ref[...].astype(jnp.float32) * HEAD_SIZE ** (-0.5)
    for h in range(pieces):
        ks[h * piece_rows : (h + 1) * piece_rows] = halo_ref[h, :, :LANES].astype(jnp.float32)
        vs[h * piece_rows : (h + 1) * piece_rows] = halo_ref[h, :, LANES:].astype(jnp.float32)
    ks[behind:] = kv_ref[:, :LANES].astype(jnp.float32)
    vs[behind:] = kv_ref[:, LANES:].astype(jnp.float32)

    passed = 0
    for number, d in enumerate(dilation_rates):
        step = min(KEYS_BEHIND, own // d)
        count = own // d // step
        span = step + KEYS_BEHIND

        def block(index, _, number=number, d=d, step=step, span=span):
            cls, b = lax.rem(index, d), index // d
            start = b * (step * d) + cls
            q_at = pl.ds(start, step, stride=d) if d > 1 else pl.ds(pl.multiple_of(start, step), step)
            k_start = behind - KEYS_BEHIND * d + start
            k_at = pl.ds(k_start, span, stride=d) if d > 1 else pl.ds(pl.multiple_of(k_start, step), span)
            q = qs[q_at, :]
            k = ks[k_at, :].astype(jnp.bfloat16)
            v = vs[k_at, :].astype(jnp.bfloat16)
            low = lax.broadcasted_iota(jnp.int32, (step, LANES), 1) < HEAD_SIZE
            q2 = jnp.concatenate([jnp.where(low, q, 0.0), jnp.where(low, 0.0, q)], axis=0).astype(jnp.bfloat16)
            s = lax.dot_general(q2, k, (((1,), (1,)), ((), ())), preferred_element_type=jnp.float32)
            row = lax.broadcasted_iota(jnp.int32, (step, span), 0)
            col = lax.broadcasted_iota(jnp.int32, (step, span), 1)
            dist = KEYS_BEHIND + row - col
            first = base // d + b * step - KEYS_BEHIND
            seen = (dist >= 0) & (dist <= KEYS_BEHIND) & (first + col >= 0)
            s = jnp.where(jnp.concatenate([seen, seen], axis=0), s, neg_big)
            top = jnp.max(s, axis=1, keepdims=True)
            p = jnp.exp(s - top)
            den = jnp.sum(p, axis=1, keepdims=True)
            o = jnp.dot(p.astype(jnp.bfloat16), v, preferred_element_type=jnp.float32)
            top = jnp.where(low, top[:step], top[step:])
            den = jnp.where(low, den[:step], den[step:])
            o = jnp.where(low, o[:step], o[step:])
            if number == 0:
                top_s[q_at, :] = top
                den_s[q_at, :] = den
                acc_s[q_at, :] = o
            else:
                was = top_s[q_at, :]
                new = jnp.maximum(was, top)
                old_scale, scale = jnp.exp(was - new), jnp.exp(top - new)
                top_s[q_at, :] = new
                den_s[q_at, :] = den_s[q_at, :] * old_scale + den * scale
                acc_s[q_at, :] = acc_s[q_at, :] * old_scale + o * scale
            return _

        lax.fori_loop(0, d * count, block, 0, unroll=2)
        if number + 1 < len(dilation_rates) and passed + 1 < planes:
            z_in(passed + 1).wait_recv()
            sides(passed + 1)
            corners(passed)
            passed += 1

    att[...] = (acc_s[...] / den_s[...]).astype(jnp.bfloat16)

    def att_out(i):
        mine = pl.ds(pl.multiple_of((g ^ i) * rows, rows), rows)
        return pltpu.make_async_remote_copy(
            src_ref=att.at[mine], dst_ref=att_all.at[g], send_sem=a_send.at[i], recv_sem=a_recv.at[i],
            device_id=at(mate(i), tp), device_id_type=MESH)

    def att_in(i):
        return pltpu.make_async_remote_copy(
            src_ref=att.at[pl.ds(0, rows)], dst_ref=att_all.at[g ^ i], send_sem=a_send.at[i], recv_sem=a_recv.at[i],
            device_id=at(mate(i), tp), device_id_type=MESH)

    def lse_out(i):
        return pltpu.make_async_remote_copy(
            src_ref=lse_ref.at[g ^ i], dst_ref=lse_all.at[g], send_sem=l_send.at[i], recv_sem=l_recv.at[i],
            device_id=at(mate(i), tp), device_id_type=MESH)

    def lse_in(i):
        return pltpu.make_async_remote_copy(
            src_ref=lse_ref.at[g ^ i], dst_ref=lse_all.at[g ^ i], send_sem=l_send.at[i], recv_sem=l_recv.at[i],
            device_id=at(mate(i), tp), device_id_type=MESH)

    for i in range(1, group):
        att_out(i).start()
    own_a = pltpu.make_async_copy(att.at[pl.ds(pl.multiple_of(g * rows, rows), rows)], att_all.at[g], own_sem.at[1])
    own_a.start()

    for t in range(own // LANES):
        at_rows = pl.ds(t * LANES, LANES)
        lse = (top_s[at_rows, :] + jnp.log(den_s[at_rows, :])).T
        b, off = (t * LANES) // rows, (t * LANES) % rows
        for h in range(heads):
            lse_ref[b, h : h + 1, off : off + LANES] = lse[h * HEAD_SIZE : h * HEAD_SIZE + 1, :]
    for i in range(1, group):
        lse_out(i).start()
    own_l = pltpu.make_async_copy(lse_ref.at[g], lse_all.at[g], own_sem.at[2])
    own_l.start()

    if group == 1:
        if planes - 1 > passed:
            lax.fori_loop(passed + 1, planes, lambda k, _: (z_in(k).wait_recv(), _)[1], 0)
    else:
        while passed + 1 < planes:
            z_in(passed + 1).wait_recv()
            sides(passed + 1)
            corners(passed)
            passed += 1
        corners(passed)
        if group == 4:
            for k in range(planes):
                for i in near:
                    corner_in(k, i).wait_recv()

    own_a.wait()
    for i in range(1, group):
        att_in(i).wait_recv()

    chunks, chunk = sums.shape[1], sums.shape[3]

    def product(c, j):
        wanted = lax.rem(tp + j, n_tp)
        here = pl.ds(pl.multiple_of(wanted * part, part), part)
        a = jnp.concatenate([att_all[b, here, :] for b in range(group)], axis=1)
        w = o_all[c * chunk : (c + 1) * chunk, :]
        return lax.dot_general(a, w, (((1,), (1,)), ((), ())), preferred_element_type=jnp.float32)

    def sum_out(c, j):
        return pltpu.make_async_remote_copy(
            src_ref=sums.at[j, c], dst_ref=sums_in.at[j, c], send_sem=s_send.at[j, c], recv_sem=s_recv.at[j, c],
            device_id=at(sp, lax.rem(tp + j, n_tp)), device_id_type=MESH)

    for j in range(1, n_tp):
        for c in range(chunks):
            sums[j, c] = product(c, j).astype(jnp.bfloat16)
            sum_out(c, j).start()
    for c in range(chunks):
        total = product(c, 0).astype(jnp.bfloat16).astype(jnp.float32)
        for j in range(1, n_tp):
            sum_out(c, j).wait_recv()
            total += sums_in[j, c].astype(jnp.float32)
        mixed_ref[:, c * chunk : (c + 1) * chunk] = total.astype(jnp.bfloat16)

    own_l.wait()
    for i in range(1, group):
        lse_in(i).wait_recv()
    for j in range(1, n_tp):
        for c in range(chunks):
            sum_out(c, j).wait_send()
    for i in range(1, group):
        att_out(i).wait_send()
        lse_out(i).wait_send()
    if planes > 1:
        lax.fori_loop(1, planes, lambda k, _: (z_out(k).wait_send(), _)[1], 0)
    if group > 1:
        for k in range(planes):
            for i in near:
                side_out(k, i).wait_send()
                if group == 4:
                    corner_out(k, i).wait_send()


def shards(n, n_tp, tokens, w_query, w_key, w_value, w_out):
    rows, model = tokens.shape
    depth, width = w_query.shape
    slabs = width // LANES
    reach = KEYS_BEHIND * dilation_rates[-1]
    group = 1
    while group < 4 and group * rows < reach and slabs % (2 * group) == 0 and n % (2 * group) == 0:
        group *= 2
    assert slabs == group
    far = (reach + group * rows - 1) // (group * rows)
    planes = n // group
    own = group * rows
    part = rows // n_tp
    heads = LANES // HEAD_SIZE

    w = jnp.stack([w_query, w_key, w_value], 1).reshape(depth, 3, group, LANES)
    w = w.transpose(2, 0, 1, 3).reshape(group, depth, 3 * LANES)

    dma = pltpu.SemaphoreType.DMA
    vmem = pl.BlockSpec(memory_space=VMEM)
    q, kv, halo = pl.pallas_call(
        functools.partial(project_kernel, n, n_tp, group, far),
        out_shape=(
            jax.ShapeDtypeStruct((own, LANES), jnp.bfloat16),
            jax.ShapeDtypeStruct((own, 2 * LANES), jnp.bfloat16),
            jax.ShapeDtypeStruct((far, own, 2 * LANES), jnp.bfloat16),
        ),
        in_specs=[vmem, pl.BlockSpec(memory_space=pl.ANY)],
        out_specs=(vmem, vmem, vmem),
        scratch_shapes=[
            VMEM((group, rows, model), jnp.bfloat16),
            VMEM((n, depth, 3 * LANES), jnp.bfloat16),
            dma((group,)), dma((group,)),
            dma((group, planes)), dma((group, planes)),
            dma((group,)), dma((group,)),
            dma((group,)), dma((group,)),
            dma((group, n_tp)), dma((group, n_tp)),
            dma((far + 1, group)), dma((far + 1, group)),
            dma((2,)),
        ],
        compiler_params=pltpu.CompilerParams(collective_id=0, has_side_effects=True, vmem_limit_bytes=48 << 20),
        cost_estimate=pl.CostEstimate(flops=2 * own * model * 3 * LANES, bytes_accessed=1 << 24, transcendentals=0),
        name="project",
    )(w, tokens)

    behind = far * own
    f32, bf16 = jnp.float32, jnp.bfloat16
    cut = w_out.shape[1]
    chunks = 4 if (n * cut) % (4 * LANES) == 0 else 1
    chunk = n * cut // chunks
    return_shapes = (
        jax.ShapeDtypeStruct((part, n * cut), bf16),
        jax.ShapeDtypeStruct((group, heads, rows), f32),
    )
    mixed, lse = pl.pallas_call(
        functools.partial(attend_kernel, n, n_tp, group, heads),
        out_shape=return_shapes,
        in_specs=[vmem] * 4,
        out_specs=(vmem, vmem),
        scratch_shapes=[
            VMEM((own, LANES), f32), VMEM((behind + own, LANES), f32), VMEM((behind + own, LANES), f32),
            VMEM((own, LANES), f32), VMEM((own, LANES), f32), VMEM((own, LANES), f32),
            VMEM((own, LANES), bf16), VMEM((group, heads, rows), f32),
            VMEM((n * cut, width), bf16), VMEM((group, rows, LANES), bf16),
            VMEM((n_tp, chunks, part, chunk), bf16), VMEM((n_tp, chunks, part, chunk), bf16),
            dma((planes,)), dma((planes,)),
            dma((planes, group)), dma((planes, group)),
            dma((planes, group)), dma((planes, group)),
            dma((group,)), dma((group,)), dma((group,)), dma((group,)),
            dma((n_tp, chunks)), dma((n_tp, chunks)),
            dma((3,)),
        ],
        compiler_params=pltpu.CompilerParams(collective_id=1, has_side_effects=True, vmem_limit_bytes=48 << 20),
        cost_estimate=pl.CostEstimate(flops=1 << 32, bytes_accessed=1 << 22, transcendentals=1 << 22),
        name="attend",
    )(q, kv, halo, w_out.T)
    return mixed, lse.reshape(group * heads, rows)


def solution(mesh):
    placed = (P("sp", None), P("sp", "tp"), P("sp", "tp"), P("sp", "tp"), P("tp", "sp"))
    return jax.shard_map(
        functools.partial(shards, mesh.shape["sp"], mesh.shape["tp"]),
        mesh=mesh,
        in_specs=placed,
        out_specs=(P(("sp", "tp"), None), P("tp", "sp")),
        check_vma=False,
    )
```

```python
import functools

import jax
import jax.numpy as jnp
from jax import lax
from jax.experimental import pallas as pl
from jax.experimental.pallas import tpu as pltpu
from jax.sharding import PartitionSpec as P

HEAD_SIZE = 64
KEYS_BEHIND = 128
LANES = 128

dilation_rates = (1, 4, 16)
neg_big = -1e30

MESH = pl.DeviceIdType.MESH
VMEM = pltpu.VMEM


def at(sp, tp):
    return {"sp": sp, "tp": tp}


def project_kernel(
    n, n_tp, group, far, wq_ref, wk_ref, wv_ref, tok_ref, o_ref, q_ref, kv_ref, halo_ref, o_plane,
    tok_all, w_all, w_ref, pack_sem, w1_send, w1_recv, up_send, up_recv, down_send, down_recv,
    t_send, t_recv, d_send, d_recv, f_send, f_recv, h_send, h_recv, o_send, o_recv, own_sem,
):
    sp, tp = lax.axis_index("sp"), lax.axis_index("tp")
    planes = n // group
    g, plane = lax.rem(sp, group), sp // group
    rows = tok_ref.shape[0]
    part = rows // n_tp
    half = part // 2

    barrier = pltpu.get_barrier_semaphore()

    def greet(j, _):
        pl.semaphore_signal(barrier, inc=1, device_id=at(lax.rem(sp + j, n), tp), device_id_type=MESH)
        return _

    lax.fori_loop(1, n, greet, 0)
    for j in range(1, n_tp):
        pl.semaphore_signal(barrier, inc=1, device_id=at(sp, lax.rem(tp + j, n_tp)), device_id_type=MESH)

    own_t = pltpu.make_async_copy(tok_ref, tok_all.at[g], own_sem.at[0])
    own_o = pltpu.make_async_copy(o_ref, o_plane.at[g], own_sem.at[1])

    def pack(t, i):
        source = (wq_ref, wk_ref, wv_ref)[t].at[:, pl.ds(pl.multiple_of((g ^ i) * LANES, LANES), LANES)]
        lanes = pl.ds(t * LANES, LANES)
        to = w_all.at[sp, :, lanes] if i == 0 else w_ref.at[i, :, lanes]
        return pltpu.make_async_copy(source, to, pack_sem.at[t, i])

    for i in list(range(1, group)) + [0]:
        for t in range(3):
            pack(t, i).start()
    own_t.start()
    own_o.start()
    pl.semaphore_wait(barrier, n - 1 + n_tp - 1)

    def mate(i):
        return plane * group + (g ^ i)

    def w_in_plane(i):
        return pltpu.make_async_remote_copy(
            src_ref=w_ref.at[i], dst_ref=w_all.at[sp], send_sem=w1_send.at[i], recv_sem=w1_recv.at[i],
            device_id=at(mate(i), tp), device_id_type=MESH)

    def w_in_plane_arrives(i):
        return pltpu.make_async_remote_copy(
            src_ref=w_ref.at[i], dst_ref=w_all.at[mate(i)], send_sem=w1_send.at[i], recv_sem=w1_recv.at[i],
            device_id=at(mate(i), tp), device_id_type=MESH)

    def slab(p, i):
        return w_all.at[lax.rem(p + 2 * planes, planes) * group + (g ^ i)]

    def up(i, k, p):
        return pltpu.make_async_remote_copy(
            src_ref=slab(p, i), dst_ref=slab(p, i), send_sem=up_send.at[i, k], recv_sem=up_recv.at[i, k],
            device_id=at(lax.rem(sp + group, n), tp), device_id_type=MESH)

    def down(i, k, p):
        return pltpu.make_async_remote_copy(
            src_ref=slab(p, i), dst_ref=slab(p, i), send_sem=down_send.at[i, k], recv_sem=down_recv.at[i, k],
            device_id=at(lax.rem(sp + n - group, n), tp), device_id_type=MESH)

    def when(condition, action):
        @pl.when(condition)
        def _():
            action()

    first, last = plane == 0, plane == planes - 1

    def relay(k, i):
        when(~last & (plane - k + 1 >= 0), lambda: up(i, k, plane - k + 1).start())
        when(~first & (plane + k - 1 < planes), lambda: down(i, k, plane + k - 1).start())

    def relayed(k, i):
        when(plane - k >= 0, lambda: up(i, k, plane - k).wait_recv())
        when(plane + k < planes, lambda: down(i, k, plane + k).wait_recv())

    def relay_left(k, i):
        when(~last & (plane - k + 1 >= 0), lambda: up(i, k, plane - k + 1).wait_send())
        when(~first & (plane + k - 1 < planes), lambda: down(i, k, plane + k - 1).wait_send())

    def hops(body):
        def one(k, _):
            for i in range(group):
                body(k, i)
            return _

        return one

    def o_out(i):
        return pltpu.make_async_remote_copy(
            src_ref=o_ref, dst_ref=o_plane.at[g], send_sem=o_send.at[i], recv_sem=o_recv.at[i],
            device_id=at(mate(i), tp), device_id_type=MESH)

    def o_in(i):
        return pltpu.make_async_remote_copy(
            src_ref=o_ref, dst_ref=o_plane.at[g ^ i], send_sem=o_send.at[i], recv_sem=o_recv.at[i],
            device_id=at(mate(i), tp), device_id_type=MESH)

    mine = pl.ds(pl.multiple_of(tp * part, part), part)

    def halves(k):
        return pl.ds(pl.multiple_of(tp * part + k * half, half), half)

    def tokens_out(i):
        return pltpu.make_async_remote_copy(
            src_ref=tok_ref.at[mine], dst_ref=tok_all.at[g, mine], send_sem=t_send.at[i], recv_sem=t_recv.at[i],
            device_id=at(mate(i), tp), device_id_type=MESH)

    def tokens_in(i):
        return pltpu.make_async_remote_copy(
            src_ref=tok_ref.at[mine], dst_ref=tok_all.at[g ^ i, mine], send_sem=t_send.at[i], recv_sem=t_recv.at[i],
            device_id=at(mate(i), tp), device_id_type=MESH)

    def corner_out(i):
        ref = tok_all.at[g ^ i, halves(i - 1)]
        return pltpu.make_async_remote_copy(
            src_ref=ref, dst_ref=ref, send_sem=d_send.at[i], recv_sem=d_recv.at[i],
            device_id=at(mate(3 - i), tp), device_id_type=MESH)

    def corner_in(i):
        ref = tok_all.at[g ^ 3, halves(i - 1)]
        return pltpu.make_async_remote_copy(
            src_ref=ref, dst_ref=ref, send_sem=d_send.at[i], recv_sem=d_recv.at[i],
            device_id=at(mate(3 - i), tp), device_id_type=MESH)

    def across(i, j):
        ref = tok_all.at[g ^ i, mine]
        return pltpu.make_async_remote_copy(
            src_ref=ref, dst_ref=ref, send_sem=f_send.at[i, j], recv_sem=f_recv.at[i, j],
            device_id=at(sp, lax.rem(tp + j, n_tp)), device_id_type=MESH)

    def across_in(i, j):
        origin = lax.rem(tp + n_tp - j, n_tp)
        ref = tok_all.at[g ^ i, pl.ds(pl.multiple_of(origin * part, part), part)]
        return pltpu.make_async_remote_copy(
            src_ref=ref, dst_ref=ref, send_sem=f_send.at[i, j], recv_sem=f_recv.at[i, j],
            device_id=at(sp, lax.rem(tp + j, n_tp)), device_id_type=MESH)

    near = [i for i in (1, 2) if i < group]
    for i in range(1, group):
        for t in range(3):
            pack(t, i).wait()
        w_in_plane(i).start()
    for t in range(3):
        pack(t, 0).wait()
    if planes > 1:
        relay(1, 0)
    for i in near:
        tokens_out(i).start()
    for i in range(1, group):
        w_in_plane_arrives(i).wait_recv()
        if planes > 1:
            relay(1, i)

    def pass_on(k, i):
        relayed(k, i)
        relay(k + 1, i)

    if planes > 1:
        lax.fori_loop(1, planes - 1, hops(pass_on), 0)
    for i in near:
        tokens_in(i).wait_recv()
        if group == 4:
            corner_out(i).start()
        for j in range(1, n_tp):
            across(i, j).start()
    for i in range(1, group):
        o_out(i).start()
    if planes > 1:
        for i in range(group):
            relayed(planes - 1, i)
    own_t.wait()

    def halo_out(h, i):
        view = pl.ds(pl.multiple_of((g ^ i) * rows, rows), rows)
        return pltpu.make_async_remote_copy(
            src_ref=kv_ref.at[view], dst_ref=halo_ref.at[far - h, view],
            send_sem=h_send.at[h, i], recv_sem=h_recv.at[h, i],
            device_id=at(lax.rem(sp + h * group, n), tp), device_id_type=MESH)

    tile = min(256, rows)

    for i in range(group):
        if i == 3:
            for k in (1, 2):
                corner_in(k).wait_recv()
            for j in range(1, n_tp):
                across(i, j).start()
        if i > 0:
            for j in range(1, n_tp):
                across_in(i, j).wait_recv()
        block = g ^ i

        def one(s, _, block=block):
            x = tok_all[block, pl.ds(pl.multiple_of(s * tile, tile), tile), :]
            w = w_all[...].reshape(-1, 3 * LANES)
            y = jnp.dot(x, w, preferred_element_type=jnp.float32).astype(jnp.bfloat16)
            to = pl.ds(pl.multiple_of(block * rows + s * tile, tile), tile)
            q_ref[to, :] = y[:, :LANES]
            kv_ref[to, :] = y[:, LANES:]
            return _

        lax.fori_loop(0, rows // tile, one, 0)
        for h in range(1, far + 1):
            @pl.when(plane + h < planes)
            def _():
                halo_out(h, i).start()

    for h in range(1, far + 1):
        @pl.when(plane - h >= 0)
        def _():
            for i in range(group):
                halo_out(h, i).wait_recv()

        @pl.when(plane - h < 0)
        def _():
            halo_ref[far - h] = jnp.zeros(halo_ref.shape[1:], halo_ref.dtype)

        @pl.when(plane + h < planes)
        def _():
            for i in range(group):
                halo_out(h, i).wait_send()

    for i in range(1, group):
        w_in_plane(i).wait_send()
        for j in range(1, n_tp):
            across(i, j).wait_send()
    for i in near:
        tokens_out(i).wait_send()
        if group == 4:
            corner_out(i).wait_send()
    if planes > 1:
        lax.fori_loop(1, planes, hops(relay_left), 0)
    own_o.wait()
    for i in range(1, group):
        o_in(i).wait_recv()
        o_out(i).wait_send()


def attend_kernel(
    n, n_tp, group, heads, q_ref, kv_ref, halo_ref, o_ref, o_plane, mixed_ref, lse_all,
    qs, ks, vs, top_s, den_s, acc_s, att, lse_ref, o_all, att_all, sums, sums_in,
    z_send, z_recv, b_send, b_recv, c_send, c_recv, a_send, a_recv, l_send, l_recv, s_send, s_recv, own_sem, o_sem,
):
    sp, tp = lax.axis_index("sp"), lax.axis_index("tp")
    planes = n // group
    g, plane = lax.rem(sp, group), sp // group
    own = q_ref.shape[0]
    base = plane * own
    rows = lse_all.shape[2]
    part = mixed_ref.shape[0]
    cut, width = o_ref.shape
    half = cut // 2

    def mate(i):
        return plane * group + (g ^ i)

    barrier = pltpu.get_barrier_semaphore()

    def greet(k, _):
        pl.semaphore_signal(barrier, inc=1, device_id=at(lax.rem(sp + k * group, n), tp), device_id_type=MESH)
        return _

    lax.fori_loop(1, planes, greet, 0)
    for i in range(1, group):
        pl.semaphore_signal(barrier, inc=1, device_id=at(mate(i), tp), device_id_type=MESH)
    for j in range(1, n_tp):
        pl.semaphore_signal(barrier, inc=1, device_id=at(sp, lax.rem(tp + j, n_tp)), device_id_type=MESH)

    def strip(k, i, part_of=None):
        origin = lax.rem(plane + planes - k, planes) * group + (g ^ i)
        if part_of is None:
            return o_all.at[pl.ds(pl.multiple_of(origin * cut, cut), cut)]
        return o_all.at[pl.ds(pl.multiple_of(origin * cut + part_of * half, half), half)]

    def z_out(k):
        return pltpu.make_async_remote_copy(
            src_ref=o_ref, dst_ref=strip(0, 0), send_sem=z_send.at[k], recv_sem=z_recv.at[k],
            device_id=at(lax.rem(sp + k * group, n), tp), device_id_type=MESH)

    def z_in(k):
        return pltpu.make_async_remote_copy(
            src_ref=o_ref, dst_ref=strip(k, 0), send_sem=z_send.at[k], recv_sem=z_recv.at[k],
            device_id=at(lax.rem(sp + k * group, n), tp), device_id_type=MESH)

    def side_out(k, i):
        return pltpu.make_async_remote_copy(
            src_ref=strip(k, 0), dst_ref=strip(k, 0), send_sem=b_send.at[k, i], recv_sem=b_recv.at[k, i],
            device_id=at(mate(i), tp), device_id_type=MESH)

    def side_in(k, i):
        return pltpu.make_async_remote_copy(
            src_ref=strip(k, i), dst_ref=strip(k, i), send_sem=b_send.at[k, i], recv_sem=b_recv.at[k, i],
            device_id=at(mate(i), tp), device_id_type=MESH)

    def corner_out(k, i):
        return pltpu.make_async_remote_copy(
            src_ref=strip(k, i, i - 1), dst_ref=strip(k, i, i - 1), send_sem=c_send.at[k, i], recv_sem=c_recv.at[k, i],
            device_id=at(mate(3 - i), tp), device_id_type=MESH)

    def corner_in(k, i):
        return pltpu.make_async_remote_copy(
            src_ref=strip(k, 3, i - 1), dst_ref=strip(k, 3, i - 1), send_sem=c_send.at[k, i], recv_sem=c_recv.at[k, i],
            device_id=at(mate(3 - i), tp), device_id_type=MESH)

    near = [i for i in (1, 2) if i < group]

    def sides(k):
        for i in near:
            side_out(k, i).start()

    def corners(k):
        for i in near:
            side_in(k, i).wait_recv()
            if group == 4:
                corner_out(k, i).start()

    def settled(i):
        return pltpu.make_async_copy(o_plane.at[g ^ i], strip(0, i), o_sem.at[i])

    for i in range(group):
        settled(i).start()
    pl.semaphore_wait(barrier, planes - 1 + group - 1 + n_tp - 1)
    if planes > 1:
        lax.fori_loop(1, planes, lambda k, _: (z_out(k).start(), _)[1], 0)

    behind = ks.shape[0] - own
    pieces, piece_rows = halo_ref.shape[0], halo_ref.shape[1]
    qs[...] = q_ref[...].astype(jnp.float32) * HEAD_SIZE ** (-0.5)
    for h in range(pieces):
        ks[h * piece_rows : (h + 1) * piece_rows] = halo_ref[h, :, :LANES].astype(jnp.float32)
        vs[h * piece_rows : (h + 1) * piece_rows] = halo_ref[h, :, LANES:].astype(jnp.float32)
    ks[behind:] = kv_ref[:, :LANES].astype(jnp.float32)
    vs[behind:] = kv_ref[:, LANES:].astype(jnp.float32)

    passed = 0
    for number, d in enumerate(dilation_rates):
        step = min(KEYS_BEHIND, own // d)
        count = own // d // step
        span = step + KEYS_BEHIND

        def block(index, _, number=number, d=d, step=step, span=span):
            cls, b = lax.rem(index, d), index // d
            start = b * (step * d) + cls
            q_at = pl.ds(start, step, stride=d) if d > 1 else pl.ds(pl.multiple_of(start, step), step)
            k_start = behind - KEYS_BEHIND * d + start
            k_at = pl.ds(k_start, span, stride=d) if d > 1 else pl.ds(pl.multiple_of(k_start, step), span)
            q = qs[q_at, :]
            k = ks[k_at, :].astype(jnp.bfloat16)
            v = vs[k_at, :].astype(jnp.bfloat16)
            low = lax.broadcasted_iota(jnp.int32, (step, LANES), 1) < HEAD_SIZE
            q2 = jnp.concatenate([jnp.where(low, q, 0.0), jnp.where(low, 0.0, q)], axis=0).astype(jnp.bfloat16)
            s = lax.dot_general(q2, k, (((1,), (1,)), ((), ())), preferred_element_type=jnp.float32)
            row = lax.broadcasted_iota(jnp.int32, (step, span), 0)
            col = lax.broadcasted_iota(jnp.int32, (step, span), 1)
            dist = KEYS_BEHIND + row - col
            first = base // d + b * step - KEYS_BEHIND
            seen = (dist >= 0) & (dist <= KEYS_BEHIND) & (first + col >= 0)
            s = jnp.where(jnp.concatenate([seen, seen], axis=0), s, neg_big)
            top = jnp.max(s, axis=1, keepdims=True)
            p = jnp.exp(s - top)
            den = jnp.sum(p, axis=1, keepdims=True)
            o = jnp.dot(p.astype(jnp.bfloat16), v, preferred_element_type=jnp.float32)
            top = jnp.where(low, top[:step], top[step:])
            den = jnp.where(low, den[:step], den[step:])
            o = jnp.where(low, o[:step], o[step:])
            if number == 0:
                top_s[q_at, :] = top
                den_s[q_at, :] = den
                acc_s[q_at, :] = o
            else:
                was = top_s[q_at, :]
                new = jnp.maximum(was, top)
                old_scale, scale = jnp.exp(was - new), jnp.exp(top - new)
                top_s[q_at, :] = new
                den_s[q_at, :] = den_s[q_at, :] * old_scale + den * scale
                acc_s[q_at, :] = acc_s[q_at, :] * old_scale + o * scale
            return _

        lax.fori_loop(0, d * count, block, 0, unroll=2)
        if number + 1 < len(dilation_rates) and passed + 1 < planes:
            z_in(passed + 1).wait_recv()
            sides(passed + 1)
            if passed > 0:
                corners(passed)
            passed += 1

    att[...] = (acc_s[...] / den_s[...]).astype(jnp.bfloat16)

    def att_out(i):
        mine = pl.ds(pl.multiple_of((g ^ i) * rows, rows), rows)
        return pltpu.make_async_remote_copy(
            src_ref=att.at[mine], dst_ref=att_all.at[g], send_sem=a_send.at[i], recv_sem=a_recv.at[i],
            device_id=at(mate(i), tp), device_id_type=MESH)

    def att_in(i):
        return pltpu.make_async_remote_copy(
            src_ref=att.at[pl.ds(0, rows)], dst_ref=att_all.at[g ^ i], send_sem=a_send.at[i], recv_sem=a_recv.at[i],
            device_id=at(mate(i), tp), device_id_type=MESH)

    def lse_out(i):
        return pltpu.make_async_remote_copy(
            src_ref=lse_ref.at[g ^ i], dst_ref=lse_all.at[g], send_sem=l_send.at[i], recv_sem=l_recv.at[i],
            device_id=at(mate(i), tp), device_id_type=MESH)

    def lse_in(i):
        return pltpu.make_async_remote_copy(
            src_ref=lse_ref.at[g ^ i], dst_ref=lse_all.at[g ^ i], send_sem=l_send.at[i], recv_sem=l_recv.at[i],
            device_id=at(mate(i), tp), device_id_type=MESH)

    for i in range(1, group):
        att_out(i).start()
    own_a = pltpu.make_async_copy(att.at[pl.ds(pl.multiple_of(g * rows, rows), rows)], att_all.at[g], own_sem.at[1])
    own_a.start()

    for t in range(own // LANES):
        at_rows = pl.ds(t * LANES, LANES)
        lse = (top_s[at_rows, :] + jnp.log(den_s[at_rows, :])).T
        b, off = (t * LANES) // rows, (t * LANES) % rows
        for h in range(heads):
            lse_ref[b, h : h + 1, off : off + LANES] = lse[h * HEAD_SIZE : h * HEAD_SIZE + 1, :]
    for i in range(1, group):
        lse_out(i).start()
    own_l = pltpu.make_async_copy(lse_ref.at[g], lse_all.at[g], own_sem.at[2])
    own_l.start()

    if group == 1:
        if planes - 1 > passed:
            lax.fori_loop(passed + 1, planes, lambda k, _: (z_in(k).wait_recv(), _)[1], 0)
    else:
        while passed + 1 < planes:
            z_in(passed + 1).wait_recv()
            sides(passed + 1)
            if passed > 0:
                corners(passed)
            passed += 1
        if passed > 0:
            corners(passed)
        if group == 4:
            for k in range(1, planes):
                for i in near:
                    corner_in(k, i).wait_recv()

    for i in range(group):
        settled(i).wait()
    own_a.wait()
    for i in range(1, group):
        att_in(i).wait_recv()

    chunks, chunk = sums.shape[1], sums.shape[3]

    def product(c, j):
        wanted = lax.rem(tp + j, n_tp)
        here = pl.ds(pl.multiple_of(wanted * part, part), part)
        a = jnp.concatenate([att_all[b, here, :] for b in range(group)], axis=1)
        w = o_all[c * chunk : (c + 1) * chunk, :]
        return lax.dot_general(a, w, (((1,), (1,)), ((), ())), preferred_element_type=jnp.float32)

    def sum_out(c, j):
        return pltpu.make_async_remote_copy(
            src_ref=sums.at[j, c], dst_ref=sums_in.at[j, c], send_sem=s_send.at[j, c], recv_sem=s_recv.at[j, c],
            device_id=at(sp, lax.rem(tp + j, n_tp)), device_id_type=MESH)

    for j in range(1, n_tp):
        for c in range(chunks):
            sums[j, c] = product(c, j).astype(jnp.bfloat16)
            sum_out(c, j).start()
    for c in range(chunks):
        total = product(c, 0).astype(jnp.bfloat16).astype(jnp.float32)
        for j in range(1, n_tp):
            sum_out(c, j).wait_recv()
            total += sums_in[j, c].astype(jnp.float32)
        mixed_ref[:, c * chunk : (c + 1) * chunk] = total.astype(jnp.bfloat16)

    own_l.wait()
    for i in range(1, group):
        lse_in(i).wait_recv()
    for j in range(1, n_tp):
        for c in range(chunks):
            sum_out(c, j).wait_send()
    for i in range(1, group):
        att_out(i).wait_send()
        lse_out(i).wait_send()
    if planes > 1:
        lax.fori_loop(1, planes, lambda k, _: (z_out(k).wait_send(), _)[1], 0)
    if group > 1:
        for k in range(1, planes):
            for i in near:
                side_out(k, i).wait_send()
                if group == 4:
                    corner_out(k, i).wait_send()


def shards(n, n_tp, tokens, w_query, w_key, w_value, w_out):
    rows, model = tokens.shape
    depth, width = w_query.shape
    slabs = width // LANES
    reach = KEYS_BEHIND * dilation_rates[-1]
    group = 1
    while group < 4 and group * rows < reach and slabs % (2 * group) == 0 and n % (2 * group) == 0:
        group *= 2
    assert slabs == group
    far = (reach + group * rows - 1) // (group * rows)
    planes = n // group
    own = group * rows
    part = rows // n_tp
    heads = LANES // HEAD_SIZE

    turned = w_out.T
    cut = w_out.shape[1]

    dma = pltpu.SemaphoreType.DMA
    vmem = pl.BlockSpec(memory_space=VMEM)
    q, kv, halo, o_plane = pl.pallas_call(
        functools.partial(project_kernel, n, n_tp, group, far),
        out_shape=(
            jax.ShapeDtypeStruct((own, LANES), jnp.bfloat16),
            jax.ShapeDtypeStruct((own, 2 * LANES), jnp.bfloat16),
            jax.ShapeDtypeStruct((far, own, 2 * LANES), jnp.bfloat16),
            jax.ShapeDtypeStruct((group, cut, width), jnp.bfloat16),
        ),
        in_specs=[pl.BlockSpec(memory_space=pl.ANY)] * 4 + [vmem],
        out_specs=(vmem,) * 4,
        scratch_shapes=[
            VMEM((group, rows, model), jnp.bfloat16),
            VMEM((n, depth, 3 * LANES), jnp.bfloat16),
            VMEM((group, depth, 3 * LANES), jnp.bfloat16),
            dma((3, group)),
            dma((group,)), dma((group,)),
            dma((group, planes)), dma((group, planes)),
            dma((group, planes)), dma((group, planes)),
            dma((group,)), dma((group,)),
            dma((group,)), dma((group,)),
            dma((group, n_tp)), dma((group, n_tp)),
            dma((far + 1, group)), dma((far + 1, group)),
            dma((group,)), dma((group,)),
            dma((2,)),
        ],
        compiler_params=pltpu.CompilerParams(collective_id=0, has_side_effects=True, vmem_limit_bytes=48 << 20),
        cost_estimate=pl.CostEstimate(flops=2 * own * model * 3 * LANES, bytes_accessed=1 << 24, transcendentals=0),
        name="project",
    )(w_query, w_key, w_value, tokens, turned)

    behind = far * own
    f32, bf16 = jnp.float32, jnp.bfloat16
    chunks = 4 if (n * cut) % (4 * LANES) == 0 else 1
    chunk = n * cut // chunks
    return_shapes = (
        jax.ShapeDtypeStruct((part, n * cut), bf16),
        jax.ShapeDtypeStruct((group, heads, rows), f32),
    )
    mixed, lse = pl.pallas_call(
        functools.partial(attend_kernel, n, n_tp, group, heads),
        out_shape=return_shapes,
        in_specs=[vmem] * 5,
        out_specs=(vmem, vmem),
        scratch_shapes=[
            VMEM((own, LANES), f32), VMEM((behind + own, LANES), f32), VMEM((behind + own, LANES), f32),
            VMEM((own, LANES), f32), VMEM((own, LANES), f32), VMEM((own, LANES), f32),
            VMEM((own, LANES), bf16), VMEM((group, heads, rows), f32),
            VMEM((n * cut, width), bf16), VMEM((group, rows, LANES), bf16),
            VMEM((n_tp, chunks, part, chunk), bf16), VMEM((n_tp, chunks, part, chunk), bf16),
            dma((planes,)), dma((planes,)),
            dma((planes, group)), dma((planes, group)),
            dma((planes, group)), dma((planes, group)),
            dma((group,)), dma((group,)), dma((group,)), dma((group,)),
            dma((n_tp, chunks)), dma((n_tp, chunks)),
            dma((3,)), dma((group,)),
        ],
        compiler_params=pltpu.CompilerParams(collective_id=1, has_side_effects=True, vmem_limit_bytes=48 << 20),
        cost_estimate=pl.CostEstimate(flops=1 << 32, bytes_accessed=1 << 22, transcendentals=1 << 22),
        name="attend",
    )(q, kv, halo, turned, o_plane)
    return mixed, lse.reshape(group * heads, rows)


def solution(mesh):
    placed = (P("sp", None), P("sp", "tp"), P("sp", "tp"), P("sp", "tp"), P("tp", "sp"))
    return jax.shard_map(
        functools.partial(shards, mesh.shape["sp"], mesh.shape["tp"]),
        mesh=mesh,
        in_specs=placed,
        out_specs=(P(("sp", "tp"), None), P("tp", "sp")),
        check_vma=False,
    )
```

```python
import functools

import jax
import jax.numpy as jnp
from jax import lax
from jax.experimental import pallas as pl
from jax.experimental.pallas import tpu as pltpu
from jax.sharding import PartitionSpec as P

HEAD_SIZE = 64
KEYS_BEHIND = 128
LANES = 128

dilation_rates = (1, 4, 16)
neg_big = -1e30

MESH = pl.DeviceIdType.MESH
VMEM = pltpu.VMEM


def at(sp, tp):
    return {"sp": sp, "tp": tp}


def project_kernel(
    n, n_tp, group, far, wq_ref, wk_ref, wv_ref, tok_ref, o_ref, q_ref, kv_ref, halo_ref, o_plane,
    tok_all, w_all, w_ref, pack_sem, w1_send, w1_recv, up_send, up_recv, down_send, down_recv,
    t_send, t_recv, d_send, d_recv, f_send, f_recv, h_send, h_recv, o_send, o_recv, own_sem,
):
    sp, tp = lax.axis_index("sp"), lax.axis_index("tp")
    planes = n // group
    g, plane = lax.rem(sp, group), sp // group
    rows = tok_ref.shape[0]
    part = rows // n_tp
    half = part // 2

    barrier = pltpu.get_barrier_semaphore()

    def greet(j, _):
        pl.semaphore_signal(barrier, inc=1, device_id=at(lax.rem(sp + j, n), tp), device_id_type=MESH)
        return _

    lax.fori_loop(1, n, greet, 0)
    for j in range(1, n_tp):
        pl.semaphore_signal(barrier, inc=1, device_id=at(sp, lax.rem(tp + j, n_tp)), device_id_type=MESH)

    own_t = pltpu.make_async_copy(tok_ref, tok_all.at[g], own_sem.at[0])
    own_o = pltpu.make_async_copy(o_ref, o_plane.at[g], own_sem.at[1])

    def pack(t, i):
        source = (wq_ref, wk_ref, wv_ref)[t].at[:, pl.ds(pl.multiple_of((g ^ i) * LANES, LANES), LANES)]
        lanes = pl.ds(t * LANES, LANES)
        to = w_all.at[sp, :, lanes] if i == 0 else w_ref.at[i, :, lanes]
        return pltpu.make_async_copy(source, to, pack_sem.at[t, i])

    for i in list(range(1, group)) + [0]:
        for t in range(3):
            pack(t, i).start()
    own_t.start()
    own_o.start()
    pl.semaphore_wait(barrier, n - 1 + n_tp - 1)

    def mate(i):
        return plane * group + (g ^ i)

    def w_in_plane(i):
        return pltpu.make_async_remote_copy(
            src_ref=w_ref.at[i], dst_ref=w_all.at[sp], send_sem=w1_send.at[i], recv_sem=w1_recv.at[i],
            device_id=at(mate(i), tp), device_id_type=MESH)

    def w_in_plane_arrives(i):
        return pltpu.make_async_remote_copy(
            src_ref=w_ref.at[i], dst_ref=w_all.at[mate(i)], send_sem=w1_send.at[i], recv_sem=w1_recv.at[i],
            device_id=at(mate(i), tp), device_id_type=MESH)

    def slab(p, i):
        return w_all.at[lax.rem(p + 2 * planes, planes) * group + (g ^ i)]

    def up(i, k, p):
        return pltpu.make_async_remote_copy(
            src_ref=slab(p, i), dst_ref=slab(p, i), send_sem=up_send.at[i, k], recv_sem=up_recv.at[i, k],
            device_id=at(lax.rem(sp + group, n), tp), device_id_type=MESH)

    def down(i, k, p):
        return pltpu.make_async_remote_copy(
            src_ref=slab(p, i), dst_ref=slab(p, i), send_sem=down_send.at[i, k], recv_sem=down_recv.at[i, k],
            device_id=at(lax.rem(sp + n - group, n), tp), device_id_type=MESH)

    def when(condition, action):
        @pl.when(condition)
        def _():
            action()

    first, last = plane == 0, plane == planes - 1

    def relay(k, i):
        when(~last & (plane - k + 1 >= 0), lambda: up(i, k, plane - k + 1).start())
        when(~first & (plane + k - 1 < planes), lambda: down(i, k, plane + k - 1).start())

    def relayed(k, i):
        when(plane - k >= 0, lambda: up(i, k, plane - k).wait_recv())
        when(plane + k < planes, lambda: down(i, k, plane + k).wait_recv())

    def relay_left(k, i):
        when(~last & (plane - k + 1 >= 0), lambda: up(i, k, plane - k + 1).wait_send())
        when(~first & (plane + k - 1 < planes), lambda: down(i, k, plane + k - 1).wait_send())

    def hops(body):
        def one(k, _):
            for i in range(group):
                body(k, i)
            return _

        return one

    def o_out(i):
        return pltpu.make_async_remote_copy(
            src_ref=o_ref, dst_ref=o_plane.at[g], send_sem=o_send.at[i], recv_sem=o_recv.at[i],
            device_id=at(mate(i), tp), device_id_type=MESH)

    def o_in(i):
        return pltpu.make_async_remote_copy(
            src_ref=o_ref, dst_ref=o_plane.at[g ^ i], send_sem=o_send.at[i], recv_sem=o_recv.at[i],
            device_id=at(mate(i), tp), device_id_type=MESH)

    mine = pl.ds(pl.multiple_of(tp * part, part), part)

    def halves(k):
        return pl.ds(pl.multiple_of(tp * part + k * half, half), half)

    def tokens_out(i):
        return pltpu.make_async_remote_copy(
            src_ref=tok_ref.at[mine], dst_ref=tok_all.at[g, mine], send_sem=t_send.at[i], recv_sem=t_recv.at[i],
            device_id=at(mate(i), tp), device_id_type=MESH)

    def tokens_in(i):
        return pltpu.make_async_remote_copy(
            src_ref=tok_ref.at[mine], dst_ref=tok_all.at[g ^ i, mine], send_sem=t_send.at[i], recv_sem=t_recv.at[i],
            device_id=at(mate(i), tp), device_id_type=MESH)

    def corner_out(i):
        ref = tok_all.at[g ^ i, halves(i - 1)]
        return pltpu.make_async_remote_copy(
            src_ref=ref, dst_ref=ref, send_sem=d_send.at[i], recv_sem=d_recv.at[i],
            device_id=at(mate(3 - i), tp), device_id_type=MESH)

    def corner_in(i):
        ref = tok_all.at[g ^ 3, halves(i - 1)]
        return pltpu.make_async_remote_copy(
            src_ref=ref, dst_ref=ref, send_sem=d_send.at[i], recv_sem=d_recv.at[i],
            device_id=at(mate(3 - i), tp), device_id_type=MESH)

    def across(i, j):
        ref = tok_all.at[g ^ i, mine]
        return pltpu.make_async_remote_copy(
            src_ref=ref, dst_ref=ref, send_sem=f_send.at[i, j], recv_sem=f_recv.at[i, j],
            device_id=at(sp, lax.rem(tp + j, n_tp)), device_id_type=MESH)

    def across_in(i, j):
        origin = lax.rem(tp + n_tp - j, n_tp)
        ref = tok_all.at[g ^ i, pl.ds(pl.multiple_of(origin * part, part), part)]
        return pltpu.make_async_remote_copy(
            src_ref=ref, dst_ref=ref, send_sem=f_send.at[i, j], recv_sem=f_recv.at[i, j],
            device_id=at(sp, lax.rem(tp + j, n_tp)), device_id_type=MESH)

    near = [i for i in (1, 2) if i < group]
    for i in range(1, group):
        for t in range(3):
            pack(t, i).wait()
        w_in_plane(i).start()
    for t in range(3):
        pack(t, 0).wait()
    if planes > 1:
        relay(1, 0)
    for i in near:
        tokens_out(i).start()
    for i in range(1, group):
        w_in_plane_arrives(i).wait_recv()
        if planes > 1:
            relay(1, i)

    def pass_on(k, i):
        relayed(k, i)
        relay(k + 1, i)

    if planes > 1:
        lax.fori_loop(1, planes - 1, hops(pass_on), 0)
    for i in near:
        tokens_in(i).wait_recv()
        if group == 4:
            corner_out(i).start()
        for j in range(1, n_tp):
            across(i, j).start()
    for i in range(1, group):
        o_out(i).start()
    if planes > 1:
        for i in range(group):
            relayed(planes - 1, i)
    own_t.wait()

    def halo_out(h, i):
        view = pl.ds(pl.multiple_of((g ^ i) * rows, rows), rows)
        return pltpu.make_async_remote_copy(
            src_ref=kv_ref.at[view], dst_ref=halo_ref.at[far - h, view],
            send_sem=h_send.at[h, i], recv_sem=h_recv.at[h, i],
            device_id=at(lax.rem(sp + h * group, n), tp), device_id_type=MESH)

    tile = min(256, rows)

    for i in range(group):
        if i == 3:
            for k in (1, 2):
                corner_in(k).wait_recv()
            for j in range(1, n_tp):
                across(i, j).start()
        if i > 0:
            for j in range(1, n_tp):
                across_in(i, j).wait_recv()
        block = g ^ i

        def one(s, _, block=block):
            x = tok_all[block, pl.ds(pl.multiple_of(s * tile, tile), tile), :]
            w = w_all[...].reshape(-1, 3 * LANES)
            y = jnp.dot(x, w, preferred_element_type=jnp.float32).astype(jnp.bfloat16)
            to = pl.ds(pl.multiple_of(block * rows + s * tile, tile), tile)
            q_ref[to, :] = y[:, :LANES]
            kv_ref[to, :] = y[:, LANES:]
            return _

        lax.fori_loop(0, rows // tile, one, 0)
        for h in range(1, far + 1):
            @pl.when(plane + h < planes)
            def _():
                halo_out(h, i).start()

    for h in range(1, far + 1):
        @pl.when(plane - h >= 0)
        def _():
            for i in range(group):
                halo_out(h, i).wait_recv()

        @pl.when(plane - h < 0)
        def _():
            halo_ref[far - h] = jnp.zeros(halo_ref.shape[1:], halo_ref.dtype)

        @pl.when(plane + h < planes)
        def _():
            for i in range(group):
                halo_out(h, i).wait_send()

    for i in range(1, group):
        w_in_plane(i).wait_send()
        for j in range(1, n_tp):
            across(i, j).wait_send()
    for i in near:
        tokens_out(i).wait_send()
        if group == 4:
            corner_out(i).wait_send()
    if planes > 1:
        lax.fori_loop(1, planes, hops(relay_left), 0)
    own_o.wait()
    for i in range(1, group):
        o_in(i).wait_recv()
        o_out(i).wait_send()


def attend_kernel(
    n, n_tp, group, heads, q_ref, kv_ref, halo_ref, o_ref, o_plane, mixed_ref, lse_all,
    qs, ks, vs, top_s, den_s, acc_s, att, lse_ref, o_all, att_all, sums, sums_in,
    z_send, z_recv, b_send, b_recv, c_send, c_recv, a_send, a_recv, l_send, l_recv, s_send, s_recv, own_sem, o_sem,
):
    sp, tp = lax.axis_index("sp"), lax.axis_index("tp")
    planes = n // group
    g, plane = lax.rem(sp, group), sp // group
    own = q_ref.shape[0]
    base = plane * own
    rows = lse_all.shape[2]
    part = mixed_ref.shape[0]
    cut, width = o_ref.shape
    half = cut // 2

    def mate(i):
        return plane * group + (g ^ i)

    barrier = pltpu.get_barrier_semaphore()

    def greet(k, _):
        pl.semaphore_signal(barrier, inc=1, device_id=at(lax.rem(sp + k * group, n), tp), device_id_type=MESH)
        return _

    lax.fori_loop(1, planes, greet, 0)
    for i in range(1, group):
        pl.semaphore_signal(barrier, inc=1, device_id=at(mate(i), tp), device_id_type=MESH)
    for j in range(1, n_tp):
        pl.semaphore_signal(barrier, inc=1, device_id=at(sp, lax.rem(tp + j, n_tp)), device_id_type=MESH)

    def strip(k, i, part_of=None):
        origin = lax.rem(plane + planes - k, planes) * group + (g ^ i)
        if part_of is None:
            return o_all.at[pl.ds(pl.multiple_of(origin * cut, cut), cut)]
        return o_all.at[pl.ds(pl.multiple_of(origin * cut + part_of * half, half), half)]

    def z_out(k):
        return pltpu.make_async_remote_copy(
            src_ref=o_ref, dst_ref=strip(0, 0), send_sem=z_send.at[k], recv_sem=z_recv.at[k],
            device_id=at(lax.rem(sp + k * group, n), tp), device_id_type=MESH)

    def z_in(k):
        return pltpu.make_async_remote_copy(
            src_ref=o_ref, dst_ref=strip(k, 0), send_sem=z_send.at[k], recv_sem=z_recv.at[k],
            device_id=at(lax.rem(sp + k * group, n), tp), device_id_type=MESH)

    def side_out(k, i):
        return pltpu.make_async_remote_copy(
            src_ref=strip(k, 0), dst_ref=strip(k, 0), send_sem=b_send.at[k, i], recv_sem=b_recv.at[k, i],
            device_id=at(mate(i), tp), device_id_type=MESH)

    def side_in(k, i):
        return pltpu.make_async_remote_copy(
            src_ref=strip(k, i), dst_ref=strip(k, i), send_sem=b_send.at[k, i], recv_sem=b_recv.at[k, i],
            device_id=at(mate(i), tp), device_id_type=MESH)

    def corner_out(k, i):
        return pltpu.make_async_remote_copy(
            src_ref=strip(k, i, i - 1), dst_ref=strip(k, i, i - 1), send_sem=c_send.at[k, i], recv_sem=c_recv.at[k, i],
            device_id=at(mate(3 - i), tp), device_id_type=MESH)

    def corner_in(k, i):
        return pltpu.make_async_remote_copy(
            src_ref=strip(k, 3, i - 1), dst_ref=strip(k, 3, i - 1), send_sem=c_send.at[k, i], recv_sem=c_recv.at[k, i],
            device_id=at(mate(3 - i), tp), device_id_type=MESH)

    near = [i for i in (1, 2) if i < group]

    def sides(k):
        for i in near:
            side_out(k, i).start()

    def corners(k):
        for i in near:
            side_in(k, i).wait_recv()
            if group == 4:
                corner_out(k, i).start()

    def settled(i):
        return pltpu.make_async_copy(o_plane.at[g ^ i], strip(0, i), o_sem.at[i])

    for i in range(group):
        settled(i).start()
    pl.semaphore_wait(barrier, planes - 1 + group - 1 + n_tp - 1)
    if planes > 1:
        lax.fori_loop(1, planes, lambda k, _: (z_out(k).start(), _)[1], 0)

    behind = ks.shape[0] - own
    pieces, piece_rows = halo_ref.shape[0], halo_ref.shape[1]
    qs[...] = q_ref[...].astype(jnp.float32) * HEAD_SIZE ** (-0.5)
    for h in range(pieces):
        ks[h * piece_rows : (h + 1) * piece_rows] = halo_ref[h, :, :LANES].astype(jnp.float32)
        vs[h * piece_rows : (h + 1) * piece_rows] = halo_ref[h, :, LANES:].astype(jnp.float32)
    ks[behind:] = kv_ref[:, :LANES].astype(jnp.float32)
    vs[behind:] = kv_ref[:, LANES:].astype(jnp.float32)

    passed = 0
    for number, d in enumerate(dilation_rates):
        step = min(KEYS_BEHIND, own // d)
        count = own // d // step
        span = step + KEYS_BEHIND

        def block(index, _, number=number, d=d, step=step, span=span):
            cls, b = lax.rem(index, d), index // d
            start = b * (step * d) + cls
            q_at = pl.ds(start, step, stride=d) if d > 1 else pl.ds(pl.multiple_of(start, step), step)
            k_start = behind - KEYS_BEHIND * d + start
            k_at = pl.ds(k_start, span, stride=d) if d > 1 else pl.ds(pl.multiple_of(k_start, step), span)
            q = qs[q_at, :]
            k = ks[k_at, :].astype(jnp.bfloat16)
            v = vs[k_at, :].astype(jnp.bfloat16)
            low = lax.broadcasted_iota(jnp.int32, (step, LANES), 1) < HEAD_SIZE
            q2 = jnp.concatenate([jnp.where(low, q, 0.0), jnp.where(low, 0.0, q)], axis=0).astype(jnp.bfloat16)
            s = lax.dot_general(q2, k, (((1,), (1,)), ((), ())), preferred_element_type=jnp.float32)
            row = lax.broadcasted_iota(jnp.int32, (step, span), 0)
            col = lax.broadcasted_iota(jnp.int32, (step, span), 1)
            dist = KEYS_BEHIND + row - col
            first = base // d + b * step - KEYS_BEHIND
            seen = (dist >= 0) & (dist <= KEYS_BEHIND) & (first + col >= 0)
            s = jnp.where(jnp.concatenate([seen, seen], axis=0), s, neg_big)
            top = jnp.max(s, axis=1, keepdims=True)
            p = jnp.exp(s - top)
            den = jnp.sum(p, axis=1, keepdims=True)
            o = jnp.dot(p.astype(jnp.bfloat16), v, preferred_element_type=jnp.float32)
            top = jnp.where(low, top[:step], top[step:])
            den = jnp.where(low, den[:step], den[step:])
            o = jnp.where(low, o[:step], o[step:])
            if number == 0:
                top_s[q_at, :] = top
                den_s[q_at, :] = den
                acc_s[q_at, :] = o
            else:
                was = top_s[q_at, :]
                new = jnp.maximum(was, top)
                old_scale, scale = jnp.exp(was - new), jnp.exp(top - new)
                top_s[q_at, :] = new
                den_s[q_at, :] = den_s[q_at, :] * old_scale + den * scale
                acc_s[q_at, :] = acc_s[q_at, :] * old_scale + o * scale
            return _

        lax.fori_loop(0, d * count, block, 0, unroll=2)
        if number + 1 < len(dilation_rates) and passed + 1 < planes:
            z_in(passed + 1).wait_recv()
            sides(passed + 1)
            if passed > 0:
                corners(passed)
            passed += 1

    att[...] = (acc_s[...] / den_s[...]).astype(jnp.bfloat16)

    def att_out(i):
        mine = pl.ds(pl.multiple_of((g ^ i) * rows, rows), rows)
        return pltpu.make_async_remote_copy(
            src_ref=att.at[mine], dst_ref=att_all.at[g], send_sem=a_send.at[i], recv_sem=a_recv.at[i],
            device_id=at(mate(i), tp), device_id_type=MESH)

    def att_in(i):
        return pltpu.make_async_remote_copy(
            src_ref=att.at[pl.ds(0, rows)], dst_ref=att_all.at[g ^ i], send_sem=a_send.at[i], recv_sem=a_recv.at[i],
            device_id=at(mate(i), tp), device_id_type=MESH)

    def lse_out(i):
        return pltpu.make_async_remote_copy(
            src_ref=lse_ref.at[g ^ i], dst_ref=lse_all.at[g], send_sem=l_send.at[i], recv_sem=l_recv.at[i],
            device_id=at(mate(i), tp), device_id_type=MESH)

    def lse_in(i):
        return pltpu.make_async_remote_copy(
            src_ref=lse_ref.at[g ^ i], dst_ref=lse_all.at[g ^ i], send_sem=l_send.at[i], recv_sem=l_recv.at[i],
            device_id=at(mate(i), tp), device_id_type=MESH)

    for i in range(1, group):
        att_out(i).start()
    own_a = pltpu.make_async_copy(att.at[pl.ds(pl.multiple_of(g * rows, rows), rows)], att_all.at[g], own_sem.at[1])
    own_a.start()

    for t in range(own // LANES):
        at_rows = pl.ds(t * LANES, LANES)
        lse = (top_s[at_rows, :] + jnp.log(den_s[at_rows, :])).T
        b, off = (t * LANES) // rows, (t * LANES) % rows
        for h in range(heads):
            lse_ref[b, h : h + 1, off : off + LANES] = lse[h * HEAD_SIZE : h * HEAD_SIZE + 1, :]
    for i in range(1, group):
        lse_out(i).start()
    own_l = pltpu.make_async_copy(lse_ref.at[g], lse_all.at[g], own_sem.at[2])
    own_l.start()

    if group == 1:
        if planes - 1 > passed:
            lax.fori_loop(passed + 1, planes, lambda k, _: (z_in(k).wait_recv(), _)[1], 0)
    else:
        while passed + 1 < planes:
            z_in(passed + 1).wait_recv()
            sides(passed + 1)
            if passed > 0:
                corners(passed)
            passed += 1
    for i in range(group):
        settled(i).wait()
    own_a.wait()
    for i in range(1, group):
        att_in(i).wait_recv()

    chunks, chunk = sums.shape[1], sums.shape[3]
    by_plane = group > 1

    def columns_of(k):
        if by_plane:
            c = lax.rem(plane + planes - k, planes)
            return pl.ds(pl.multiple_of(c * chunk, chunk), chunk)
        return pl.ds(k * chunk, chunk)

    def product(c, j):
        wanted = lax.rem(tp + j, n_tp)
        here = pl.ds(pl.multiple_of(wanted * part, part), part)
        a = jnp.concatenate([att_all[b, here, :] for b in range(group)], axis=1)
        w = o_all[columns_of(c), :]
        return lax.dot_general(a, w, (((1,), (1,)), ((), ())), preferred_element_type=jnp.float32)

    def sum_out(c, j):
        return pltpu.make_async_remote_copy(
            src_ref=sums.at[j, c], dst_ref=sums_in.at[j, c], send_sem=s_send.at[j, c], recv_sem=s_recv.at[j, c],
            device_id=at(sp, lax.rem(tp + j, n_tp)), device_id_type=MESH)

    def for_others(c):
        for j in range(1, n_tp):
            sums[j, c] = product(c, j).astype(jnp.bfloat16)
            sum_out(c, j).start()

    def for_self(c):
        total = product(c, 0).astype(jnp.bfloat16).astype(jnp.float32)
        for j in range(1, n_tp):
            sum_out(c, j).wait_recv()
            total += sums_in[j, c].astype(jnp.float32)
        mixed_ref[:, columns_of(c)] = total.astype(jnp.bfloat16)

    for c in range(chunks):
        if group == 4 and c > 0:
            for i in near:
                corner_in(c, i).wait_recv()
        for_others(c)
        if by_plane and c == 0 and passed > 0:
            corners(passed)
        if 0 < c < chunks - 1:
            for_self(c - 1)
    if chunks > 1:
        for_self(chunks - 2)
    for_self(chunks - 1)

    own_l.wait()
    for i in range(1, group):
        lse_in(i).wait_recv()
    for j in range(1, n_tp):
        for c in range(chunks):
            sum_out(c, j).wait_send()
    for i in range(1, group):
        att_out(i).wait_send()
        lse_out(i).wait_send()
    if planes > 1:
        lax.fori_loop(1, planes, lambda k, _: (z_out(k).wait_send(), _)[1], 0)
    if group > 1:
        for k in range(1, planes):
            for i in near:
                side_out(k, i).wait_send()
                if group == 4:
                    corner_out(k, i).wait_send()


def shards(n, n_tp, tokens, w_query, w_key, w_value, w_out):
    rows, model = tokens.shape
    depth, width = w_query.shape
    slabs = width // LANES
    reach = KEYS_BEHIND * dilation_rates[-1]
    group = 1
    while group < 4 and group * rows < reach and slabs % (2 * group) == 0 and n % (2 * group) == 0:
        group *= 2
    assert slabs == group
    far = (reach + group * rows - 1) // (group * rows)
    planes = n // group
    own = group * rows
    part = rows // n_tp
    heads = LANES // HEAD_SIZE

    turned = w_out.T
    cut = w_out.shape[1]

    dma = pltpu.SemaphoreType.DMA
    vmem = pl.BlockSpec(memory_space=VMEM)
    q, kv, halo, o_plane = pl.pallas_call(
        functools.partial(project_kernel, n, n_tp, group, far),
        out_shape=(
            jax.ShapeDtypeStruct((own, LANES), jnp.bfloat16),
            jax.ShapeDtypeStruct((own, 2 * LANES), jnp.bfloat16),
            jax.ShapeDtypeStruct((far, own, 2 * LANES), jnp.bfloat16),
            jax.ShapeDtypeStruct((group, cut, width), jnp.bfloat16),
        ),
        in_specs=[pl.BlockSpec(memory_space=pltpu.HBM)] * 4 + [vmem],
        out_specs=(vmem,) * 4,
        scratch_shapes=[
            VMEM((group, rows, model), jnp.bfloat16),
            VMEM((n, depth, 3 * LANES), jnp.bfloat16),
            VMEM((group, depth, 3 * LANES), jnp.bfloat16),
            dma((3, group)),
            dma((group,)), dma((group,)),
            dma((group, planes)), dma((group, planes)),
            dma((group, planes)), dma((group, planes)),
            dma((group,)), dma((group,)),
            dma((group,)), dma((group,)),
            dma((group, n_tp)), dma((group, n_tp)),
            dma((far + 1, group)), dma((far + 1, group)),
            dma((group,)), dma((group,)),
            dma((2,)),
        ],
        compiler_params=pltpu.CompilerParams(collective_id=0, has_side_effects=True, vmem_limit_bytes=48 << 20),
        cost_estimate=pl.CostEstimate(flops=2 * own * model * 3 * LANES, bytes_accessed=1 << 24, transcendentals=0),
        name="project",
    )(w_query, w_key, w_value, tokens, turned)

    behind = far * own
    f32, bf16 = jnp.float32, jnp.bfloat16
    chunks = planes if group > 1 else (4 if (n * cut) % (4 * LANES) == 0 else 1)
    chunk = n * cut // chunks
    return_shapes = (
        jax.ShapeDtypeStruct((part, n * cut), bf16),
        jax.ShapeDtypeStruct((group, heads, rows), f32),
    )
    mixed, lse = pl.pallas_call(
        functools.partial(attend_kernel, n, n_tp, group, heads),
        out_shape=return_shapes,
        in_specs=[vmem] * 5,
        out_specs=(vmem, vmem),
        scratch_shapes=[
            VMEM((own, LANES), f32), VMEM((behind + own, LANES), f32), VMEM((behind + own, LANES), f32),
            VMEM((own, LANES), f32), VMEM((own, LANES), f32), VMEM((own, LANES), f32),
            VMEM((own, LANES), bf16), VMEM((group, heads, rows), f32),
            VMEM((n * cut, width), bf16), VMEM((group, rows, LANES), bf16),
            VMEM((n_tp, chunks, part, chunk), bf16), VMEM((n_tp, chunks, part, chunk), bf16),
            dma((planes,)), dma((planes,)),
            dma((planes, group)), dma((planes, group)),
            dma((planes, group)), dma((planes, group)),
            dma((group,)), dma((group,)), dma((group,)), dma((group,)),
            dma((n_tp, chunks)), dma((n_tp, chunks)),
            dma((3,)), dma((group,)),
        ],
        compiler_params=pltpu.CompilerParams(collective_id=1, has_side_effects=True, vmem_limit_bytes=48 << 20),
        cost_estimate=pl.CostEstimate(flops=1 << 32, bytes_accessed=1 << 22, transcendentals=1 << 22),
        name="attend",
    )(q, kv, halo, turned, o_plane)
    return mixed, lse.reshape(group * heads, rows)


def solution(mesh):
    placed = (P("sp", None), P("sp", "tp"), P("sp", "tp"), P("sp", "tp"), P("tp", "sp"))
    return jax.shard_map(
        functools.partial(shards, mesh.shape["sp"], mesh.shape["tp"]),
        mesh=mesh,
        in_specs=placed,
        out_specs=(P(("sp", "tp"), None), P("tp", "sp")),
        check_vma=False,
    )
```

```python
import functools

import jax
import jax.numpy as jnp
from jax import lax
from jax.experimental import pallas as pl
from jax.experimental.pallas import tpu as pltpu
from jax.sharding import PartitionSpec as P

HEAD_SIZE = 64
KEYS_BEHIND = 128
LANES = 128

dilation_rates = (1, 4, 16)
neg_big = -1e30

MESH = pl.DeviceIdType.MESH
VMEM = pltpu.VMEM


def at(sp, tp):
    return {"sp": sp, "tp": tp}


def project_kernel(
    n, n_tp, group, far, wq_ref, wk_ref, wv_ref, tok_ref, o_ref, q_ref, kv_ref, halo_ref, o_plane, o_far,
    tok_all, w_all, w_ref, pack_sem, w1_send, w1_recv, up_send, up_recv, down_send, down_recv,
    t_send, t_recv, d_send, d_recv, f_send, f_recv, h_send, h_recv, o_send, o_recv, z_send, z_recv, own_sem,
):
    sp, tp = lax.axis_index("sp"), lax.axis_index("tp")
    planes = n // group
    g, plane = lax.rem(sp, group), sp // group
    rows = tok_ref.shape[0]
    part = rows // n_tp
    half = part // 2

    barrier = pltpu.get_barrier_semaphore()

    def greet(j, _):
        pl.semaphore_signal(barrier, inc=1, device_id=at(lax.rem(sp + j, n), tp), device_id_type=MESH)
        return _

    lax.fori_loop(1, n, greet, 0)
    for j in range(1, n_tp):
        pl.semaphore_signal(barrier, inc=1, device_id=at(sp, lax.rem(tp + j, n_tp)), device_id_type=MESH)

    own_t = pltpu.make_async_copy(tok_ref, tok_all.at[g], own_sem.at[0])
    own_o = pltpu.make_async_copy(o_ref, o_plane.at[g], own_sem.at[1])

    def pack(t, i):
        source = (wq_ref, wk_ref, wv_ref)[t].at[:, pl.ds(pl.multiple_of((g ^ i) * LANES, LANES), LANES)]
        lanes = pl.ds(t * LANES, LANES)
        to = w_all.at[sp, :, lanes] if i == 0 else w_ref.at[i, :, lanes]
        return pltpu.make_async_copy(source, to, pack_sem.at[t, i])

    for i in list(range(1, group)) + [0]:
        for t in range(3):
            pack(t, i).start()
    own_t.start()
    own_o.start()
    pl.semaphore_wait(barrier, n - 1 + n_tp - 1)

    def mate(i):
        return plane * group + (g ^ i)

    def w_in_plane(i):
        return pltpu.make_async_remote_copy(
            src_ref=w_ref.at[i], dst_ref=w_all.at[sp], send_sem=w1_send.at[i], recv_sem=w1_recv.at[i],
            device_id=at(mate(i), tp), device_id_type=MESH)

    def w_in_plane_arrives(i):
        return pltpu.make_async_remote_copy(
            src_ref=w_ref.at[i], dst_ref=w_all.at[mate(i)], send_sem=w1_send.at[i], recv_sem=w1_recv.at[i],
            device_id=at(mate(i), tp), device_id_type=MESH)

    def slab(p, i):
        return w_all.at[lax.rem(p + 2 * planes, planes) * group + (g ^ i)]

    def up(i, k, p):
        return pltpu.make_async_remote_copy(
            src_ref=slab(p, i), dst_ref=slab(p, i), send_sem=up_send.at[i, k], recv_sem=up_recv.at[i, k],
            device_id=at(lax.rem(sp + group, n), tp), device_id_type=MESH)

    def down(i, k, p):
        return pltpu.make_async_remote_copy(
            src_ref=slab(p, i), dst_ref=slab(p, i), send_sem=down_send.at[i, k], recv_sem=down_recv.at[i, k],
            device_id=at(lax.rem(sp + n - group, n), tp), device_id_type=MESH)

    def when(condition, action):
        @pl.when(condition)
        def _():
            action()

    first, last = plane == 0, plane == planes - 1

    def relay(k, i):
        when(~last & (plane - k + 1 >= 0), lambda: up(i, k, plane - k + 1).start())
        when(~first & (plane + k - 1 < planes), lambda: down(i, k, plane + k - 1).start())

    def relayed(k, i):
        when(plane - k >= 0, lambda: up(i, k, plane - k).wait_recv())
        when(plane + k < planes, lambda: down(i, k, plane + k).wait_recv())

    def relay_left(k, i):
        when(~last & (plane - k + 1 >= 0), lambda: up(i, k, plane - k + 1).wait_send())
        when(~first & (plane + k - 1 < planes), lambda: down(i, k, plane + k - 1).wait_send())

    def hops(body):
        def one(k, _):
            for i in range(group):
                body(k, i)
            return _

        return one

    def o_out(i):
        return pltpu.make_async_remote_copy(
            src_ref=o_ref, dst_ref=o_plane.at[g], send_sem=o_send.at[i], recv_sem=o_recv.at[i],
            device_id=at(mate(i), tp), device_id_type=MESH)

    def o_in(i):
        return pltpu.make_async_remote_copy(
            src_ref=o_ref, dst_ref=o_plane.at[g ^ i], send_sem=o_send.at[i], recv_sem=o_recv.at[i],
            device_id=at(mate(i), tp), device_id_type=MESH)

    mine = pl.ds(pl.multiple_of(tp * part, part), part)

    def halves(k):
        return pl.ds(pl.multiple_of(tp * part + k * half, half), half)

    def tokens_out(i):
        return pltpu.make_async_remote_copy(
            src_ref=tok_ref.at[mine], dst_ref=tok_all.at[g, mine], send_sem=t_send.at[i], recv_sem=t_recv.at[i],
            device_id=at(mate(i), tp), device_id_type=MESH)

    def tokens_in(i):
        return pltpu.make_async_remote_copy(
            src_ref=tok_ref.at[mine], dst_ref=tok_all.at[g ^ i, mine], send_sem=t_send.at[i], recv_sem=t_recv.at[i],
            device_id=at(mate(i), tp), device_id_type=MESH)

    def corner_out(i):
        ref = tok_all.at[g ^ i, halves(i - 1)]
        return pltpu.make_async_remote_copy(
            src_ref=ref, dst_ref=ref, send_sem=d_send.at[i], recv_sem=d_recv.at[i],
            device_id=at(mate(3 - i), tp), device_id_type=MESH)

    def corner_in(i):
        ref = tok_all.at[g ^ 3, halves(i - 1)]
        return pltpu.make_async_remote_copy(
            src_ref=ref, dst_ref=ref, send_sem=d_send.at[i], recv_sem=d_recv.at[i],
            device_id=at(mate(3 - i), tp), device_id_type=MESH)

    def across(i, j):
        ref = tok_all.at[g ^ i, mine]
        return pltpu.make_async_remote_copy(
            src_ref=ref, dst_ref=ref, send_sem=f_send.at[i, j], recv_sem=f_recv.at[i, j],
            device_id=at(sp, lax.rem(tp + j, n_tp)), device_id_type=MESH)

    def across_in(i, j):
        origin = lax.rem(tp + n_tp - j, n_tp)
        ref = tok_all.at[g ^ i, pl.ds(pl.multiple_of(origin * part, part), part)]
        return pltpu.make_async_remote_copy(
            src_ref=ref, dst_ref=ref, send_sem=f_send.at[i, j], recv_sem=f_recv.at[i, j],
            device_id=at(sp, lax.rem(tp + j, n_tp)), device_id_type=MESH)

    near = [i for i in (1, 2) if i < group]
    def z_out(k):
        return pltpu.make_async_remote_copy(
            src_ref=o_ref, dst_ref=o_far.at[k], send_sem=z_send.at[k], recv_sem=z_recv.at[k],
            device_id=at(lax.rem(sp + k * group, n), tp), device_id_type=MESH)

    for i in range(1, group):
        for t in range(3):
            pack(t, i).wait()
        w_in_plane(i).start()
    for t in range(3):
        pack(t, 0).wait()
    if planes > 1:
        relay(1, 0)
    for i in near:
        tokens_out(i).start()
    for i in range(1, group):
        w_in_plane_arrives(i).wait_recv()
        if planes > 1:
            relay(1, i)

    def pass_on(k, i):
        relayed(k, i)
        relay(k + 1, i)

    if planes > 1:
        lax.fori_loop(1, planes, lambda k, _: (z_out(k).start(), _)[1], 0)
        lax.fori_loop(1, planes - 1, hops(pass_on), 0)
    for i in near:
        tokens_in(i).wait_recv()
        if group == 4:
            corner_out(i).start()
        for j in range(1, n_tp):
            across(i, j).start()
    for i in range(1, group):
        o_out(i).start()
    if planes > 1:
        for i in range(group):
            relayed(planes - 1, i)
    own_t.wait()

    def halo_out(h, i):
        view = pl.ds(pl.multiple_of((g ^ i) * rows, rows), rows)
        return pltpu.make_async_remote_copy(
            src_ref=kv_ref.at[view], dst_ref=halo_ref.at[far - h, view],
            send_sem=h_send.at[h, i], recv_sem=h_recv.at[h, i],
            device_id=at(lax.rem(sp + h * group, n), tp), device_id_type=MESH)

    tile = min(256, rows)

    for i in range(group):
        if i == 3:
            for k in (1, 2):
                corner_in(k).wait_recv()
            for j in range(1, n_tp):
                across(i, j).start()
        if i > 0:
            for j in range(1, n_tp):
                across_in(i, j).wait_recv()
        block = g ^ i

        def one(s, _, block=block):
            x = tok_all[block, pl.ds(pl.multiple_of(s * tile, tile), tile), :]
            w = w_all[...].reshape(-1, 3 * LANES)
            y = jnp.dot(x, w, preferred_element_type=jnp.float32).astype(jnp.bfloat16)
            to = pl.ds(pl.multiple_of(block * rows + s * tile, tile), tile)
            q_ref[to, :] = y[:, :LANES]
            kv_ref[to, :] = y[:, LANES:]
            return _

        lax.fori_loop(0, rows // tile, one, 0)
        for h in range(1, far + 1):
            @pl.when(plane + h < planes)
            def _():
                halo_out(h, i).start()

    for h in range(1, far + 1):
        @pl.when(plane - h >= 0)
        def _():
            for i in range(group):
                halo_out(h, i).wait_recv()

        @pl.when(plane - h < 0)
        def _():
            halo_ref[far - h] = jnp.zeros(halo_ref.shape[1:], halo_ref.dtype)

        @pl.when(plane + h < planes)
        def _():
            for i in range(group):
                halo_out(h, i).wait_send()

    for i in range(1, group):
        w_in_plane(i).wait_send()
        for j in range(1, n_tp):
            across(i, j).wait_send()
    for i in near:
        tokens_out(i).wait_send()
        if group == 4:
            corner_out(i).wait_send()
    if planes > 1:
        lax.fori_loop(1, planes, hops(relay_left), 0)
        lax.fori_loop(1, planes, lambda k, _: (z_out(k).wait(), _)[1], 0)
    own_o.wait()
    for i in range(1, group):
        o_in(i).wait_recv()
        o_out(i).wait_send()


def attend_kernel(
    n, n_tp, group, heads, q_ref, kv_ref, halo_ref, o_far, o_plane, mixed_ref, lse_all,
    qs, ks, vs, top_s, den_s, acc_s, att, lse_ref, o_all, att_all, sums, sums_in,
    z_recv, b_send, b_recv, c_send, c_recv, a_send, a_recv, l_send, l_recv, s_send, s_recv, own_sem, o_sem,
):
    sp, tp = lax.axis_index("sp"), lax.axis_index("tp")
    planes = n // group
    g, plane = lax.rem(sp, group), sp // group
    own = q_ref.shape[0]
    base = plane * own
    rows = lse_all.shape[2]
    part = mixed_ref.shape[0]
    cut, width = o_plane.shape[1:]
    half = cut // 2

    def mate(i):
        return plane * group + (g ^ i)

    barrier = pltpu.get_barrier_semaphore()

    for i in range(1, group):
        pl.semaphore_signal(barrier, inc=1, device_id=at(mate(i), tp), device_id_type=MESH)
    for j in range(1, n_tp):
        pl.semaphore_signal(barrier, inc=1, device_id=at(sp, lax.rem(tp + j, n_tp)), device_id_type=MESH)

    def strip(k, i, part_of=None):
        origin = lax.rem(plane + planes - k, planes) * group + (g ^ i)
        if part_of is None:
            return o_all.at[pl.ds(pl.multiple_of(origin * cut, cut), cut)]
        return o_all.at[pl.ds(pl.multiple_of(origin * cut + part_of * half, half), half)]

    def z_in(k):
        return pltpu.make_async_copy(o_far.at[k], strip(k, 0), z_recv.at[k])

    def side_out(k, i):
        return pltpu.make_async_remote_copy(
            src_ref=o_far.at[k], dst_ref=strip(k, 0), send_sem=b_send.at[k, i], recv_sem=b_recv.at[k, i],
            device_id=at(mate(i), tp), device_id_type=MESH)

    def side_in(k, i):
        return pltpu.make_async_remote_copy(
            src_ref=strip(k, i), dst_ref=strip(k, i), send_sem=b_send.at[k, i], recv_sem=b_recv.at[k, i],
            device_id=at(mate(i), tp), device_id_type=MESH)

    def corner_out(k, i):
        return pltpu.make_async_remote_copy(
            src_ref=strip(k, i, i - 1), dst_ref=strip(k, i, i - 1), send_sem=c_send.at[k, i], recv_sem=c_recv.at[k, i],
            device_id=at(mate(3 - i), tp), device_id_type=MESH)

    def corner_in(k, i):
        return pltpu.make_async_remote_copy(
            src_ref=strip(k, 3, i - 1), dst_ref=strip(k, 3, i - 1), send_sem=c_send.at[k, i], recv_sem=c_recv.at[k, i],
            device_id=at(mate(3 - i), tp), device_id_type=MESH)

    near = [i for i in (1, 2) if i < group]

    def sides(k):
        for i in near:
            side_out(k, i).start()

    def corners(k):
        for i in near:
            side_in(k, i).wait_recv()
            if group == 4:
                corner_out(k, i).start()

    def settled(i):
        return pltpu.make_async_copy(o_plane.at[g ^ i], strip(0, i), o_sem.at[i])

    for i in range(group):
        settled(i).start()
    if planes > 1:
        lax.fori_loop(1, planes, lambda k, _: (z_in(k).start(), _)[1], 0)
    pl.semaphore_wait(barrier, group - 1 + n_tp - 1)
    if group > 1:
        for k in range(1, planes):
            sides(k)

    behind = ks.shape[0] - own
    pieces, piece_rows = halo_ref.shape[0], halo_ref.shape[1]
    qs[...] = q_ref[...].astype(jnp.float32) * HEAD_SIZE ** (-0.5)
    for h in range(pieces):
        ks[h * piece_rows : (h + 1) * piece_rows] = halo_ref[h, :, :LANES].astype(jnp.float32)
        vs[h * piece_rows : (h + 1) * piece_rows] = halo_ref[h, :, LANES:].astype(jnp.float32)
    ks[behind:] = kv_ref[:, :LANES].astype(jnp.float32)
    vs[behind:] = kv_ref[:, LANES:].astype(jnp.float32)

    passed = 0
    for number, d in enumerate(dilation_rates):
        step = min(KEYS_BEHIND, own // d)
        count = own // d // step
        span = step + KEYS_BEHIND

        def block(index, _, number=number, d=d, step=step, span=span):
            cls, b = lax.rem(index, d), index // d
            start = b * (step * d) + cls
            q_at = pl.ds(start, step, stride=d) if d > 1 else pl.ds(pl.multiple_of(start, step), step)
            k_start = behind - KEYS_BEHIND * d + start
            k_at = pl.ds(k_start, span, stride=d) if d > 1 else pl.ds(pl.multiple_of(k_start, step), span)
            q = qs[q_at, :]
            k = ks[k_at, :].astype(jnp.bfloat16)
            v = vs[k_at, :].astype(jnp.bfloat16)
            low = lax.broadcasted_iota(jnp.int32, (step, LANES), 1) < HEAD_SIZE
            q2 = jnp.concatenate([jnp.where(low, q, 0.0), jnp.where(low, 0.0, q)], axis=0).astype(jnp.bfloat16)
            s = lax.dot_general(q2, k, (((1,), (1,)), ((), ())), preferred_element_type=jnp.float32)
            row = lax.broadcasted_iota(jnp.int32, (step, span), 0)
            col = lax.broadcasted_iota(jnp.int32, (step, span), 1)
            dist = KEYS_BEHIND + row - col
            first = base // d + b * step - KEYS_BEHIND
            seen = (dist >= 0) & (dist <= KEYS_BEHIND) & (first + col >= 0)
            s = jnp.where(jnp.concatenate([seen, seen], axis=0), s, neg_big)
            top = jnp.max(s, axis=1, keepdims=True)
            p = jnp.exp(s - top)
            den = jnp.sum(p, axis=1, keepdims=True)
            o = jnp.dot(p.astype(jnp.bfloat16), v, preferred_element_type=jnp.float32)
            top = jnp.where(low, top[:step], top[step:])
            den = jnp.where(low, den[:step], den[step:])
            o = jnp.where(low, o[:step], o[step:])
            if number == 0:
                top_s[q_at, :] = top
                den_s[q_at, :] = den
                acc_s[q_at, :] = o
            else:
                was = top_s[q_at, :]
                new = jnp.maximum(was, top)
                old_scale, scale = jnp.exp(was - new), jnp.exp(top - new)
                top_s[q_at, :] = new
                den_s[q_at, :] = den_s[q_at, :] * old_scale + den * scale
                acc_s[q_at, :] = acc_s[q_at, :] * old_scale + o * scale
            return _

        lax.fori_loop(0, d * count, block, 0, unroll=2)
        if number + 1 < len(dilation_rates) and passed + 1 < planes:
            passed += 1
            corners(passed)

    att[...] = (acc_s[...] / den_s[...]).astype(jnp.bfloat16)

    def att_out(i):
        mine = pl.ds(pl.multiple_of((g ^ i) * rows, rows), rows)
        return pltpu.make_async_remote_copy(
            src_ref=att.at[mine], dst_ref=att_all.at[g], send_sem=a_send.at[i], recv_sem=a_recv.at[i],
            device_id=at(mate(i), tp), device_id_type=MESH)

    def att_in(i):
        return pltpu.make_async_remote_copy(
            src_ref=att.at[pl.ds(0, rows)], dst_ref=att_all.at[g ^ i], send_sem=a_send.at[i], recv_sem=a_recv.at[i],
            device_id=at(mate(i), tp), device_id_type=MESH)

    def lse_out(i):
        return pltpu.make_async_remote_copy(
            src_ref=lse_ref.at[g ^ i], dst_ref=lse_all.at[g], send_sem=l_send.at[i], recv_sem=l_recv.at[i],
            device_id=at(mate(i), tp), device_id_type=MESH)

    def lse_in(i):
        return pltpu.make_async_remote_copy(
            src_ref=lse_ref.at[g ^ i], dst_ref=lse_all.at[g ^ i], send_sem=l_send.at[i], recv_sem=l_recv.at[i],
            device_id=at(mate(i), tp), device_id_type=MESH)

    for i in range(1, group):
        att_out(i).start()
    own_a = pltpu.make_async_copy(att.at[pl.ds(pl.multiple_of(g * rows, rows), rows)], att_all.at[g], own_sem.at[1])
    own_a.start()

    for t in range(own // LANES):
        at_rows = pl.ds(t * LANES, LANES)
        lse = (top_s[at_rows, :] + jnp.log(den_s[at_rows, :])).T
        b, off = (t * LANES) // rows, (t * LANES) % rows
        for h in range(heads):
            lse_ref[b, h : h + 1, off : off + LANES] = lse[h * HEAD_SIZE : h * HEAD_SIZE + 1, :]
    for i in range(1, group):
        lse_out(i).start()
    own_l = pltpu.make_async_copy(lse_ref.at[g], lse_all.at[g], own_sem.at[2])
    own_l.start()

    while group > 1 and passed + 1 < planes:
        passed += 1
        corners(passed)
    if planes > 1:
        lax.fori_loop(1, planes, lambda k, _: (z_in(k).wait(), _)[1], 0)
    for i in range(group):
        settled(i).wait()
    own_a.wait()
    for i in range(1, group):
        att_in(i).wait_recv()

    chunks, chunk = sums.shape[1], sums.shape[3]
    by_plane = group > 1

    def columns_of(k):
        if by_plane:
            c = lax.rem(plane + planes - k, planes)
            return pl.ds(pl.multiple_of(c * chunk, chunk), chunk)
        return pl.ds(k * chunk, chunk)

    def product(c, j):
        wanted = lax.rem(tp + j, n_tp)
        here = pl.ds(pl.multiple_of(wanted * part, part), part)
        a = jnp.concatenate([att_all[b, here, :] for b in range(group)], axis=1)
        w = o_all[columns_of(c), :]
        return lax.dot_general(a, w, (((1,), (1,)), ((), ())), preferred_element_type=jnp.float32)

    def sum_out(c, j):
        return pltpu.make_async_remote_copy(
            src_ref=sums.at[j, c], dst_ref=sums_in.at[j, c], send_sem=s_send.at[j, c], recv_sem=s_recv.at[j, c],
            device_id=at(sp, lax.rem(tp + j, n_tp)), device_id_type=MESH)

    def for_others(c):
        for j in range(1, n_tp):
            sums[j, c] = product(c, j).astype(jnp.bfloat16)
            sum_out(c, j).start()

    def for_self(c):
        total = product(c, 0).astype(jnp.bfloat16).astype(jnp.float32)
        for j in range(1, n_tp):
            sum_out(c, j).wait_recv()
            total += sums_in[j, c].astype(jnp.float32)
        mixed_ref[:, columns_of(c)] = total.astype(jnp.bfloat16)

    for c in range(chunks):
        if group == 4 and c > 0:
            for i in near:
                corner_in(c, i).wait_recv()
        for_others(c)
        if 0 < c < chunks - 1:
            for_self(c - 1)
    if chunks > 1:
        for_self(chunks - 2)
    for_self(chunks - 1)

    own_l.wait()
    for i in range(1, group):
        lse_in(i).wait_recv()
    for j in range(1, n_tp):
        for c in range(chunks):
            sum_out(c, j).wait_send()
    for i in range(1, group):
        att_out(i).wait_send()
        lse_out(i).wait_send()
    if group > 1:
        for k in range(1, planes):
            for i in near:
                side_out(k, i).wait_send()
                if group == 4:
                    corner_out(k, i).wait_send()


def shards(n, n_tp, tokens, w_query, w_key, w_value, w_out):
    rows, model = tokens.shape
    depth, width = w_query.shape
    slabs = width // LANES
    reach = KEYS_BEHIND * dilation_rates[-1]
    group = 1
    while group < 4 and group * rows < reach and slabs % (2 * group) == 0 and n % (2 * group) == 0:
        group *= 2
    assert slabs == group
    far = (reach + group * rows - 1) // (group * rows)
    planes = n // group
    own = group * rows
    part = rows // n_tp
    heads = LANES // HEAD_SIZE

    turned = w_out.T
    cut = w_out.shape[1]

    dma = pltpu.SemaphoreType.DMA
    vmem = pl.BlockSpec(memory_space=VMEM)
    q, kv, halo, o_plane, o_far = pl.pallas_call(
        functools.partial(project_kernel, n, n_tp, group, far),
        out_shape=(
            jax.ShapeDtypeStruct((own, LANES), jnp.bfloat16),
            jax.ShapeDtypeStruct((own, 2 * LANES), jnp.bfloat16),
            jax.ShapeDtypeStruct((far, own, 2 * LANES), jnp.bfloat16),
            jax.ShapeDtypeStruct((group, cut, width), jnp.bfloat16),
            jax.ShapeDtypeStruct((planes, cut, width), jnp.bfloat16),
        ),
        in_specs=[pl.BlockSpec(memory_space=pltpu.HBM)] * 4 + [vmem],
        out_specs=(vmem,) * 5,
        scratch_shapes=[
            VMEM((group, rows, model), jnp.bfloat16),
            VMEM((n, depth, 3 * LANES), jnp.bfloat16),
            VMEM((group, depth, 3 * LANES), jnp.bfloat16),
            dma((3, group)),
            dma((group,)), dma((group,)),
            dma((group, planes)), dma((group, planes)),
            dma((group, planes)), dma((group, planes)),
            dma((group,)), dma((group,)),
            dma((group,)), dma((group,)),
            dma((group, n_tp)), dma((group, n_tp)),
            dma((far + 1, group)), dma((far + 1, group)),
            dma((group,)), dma((group,)), dma((planes,)), dma((planes,)),
            dma((2,)),
        ],
        compiler_params=pltpu.CompilerParams(collective_id=0, has_side_effects=True, vmem_limit_bytes=48 << 20),
        cost_estimate=pl.CostEstimate(flops=2 * own * model * 3 * LANES, bytes_accessed=1 << 24, transcendentals=0),
        name="project",
    )(w_query, w_key, w_value, tokens, turned)

    behind = far * own
    f32, bf16 = jnp.float32, jnp.bfloat16
    chunks = planes if group > 1 else (4 if (n * cut) % (4 * LANES) == 0 else 1)
    chunk = n * cut // chunks
    return_shapes = (
        jax.ShapeDtypeStruct((part, n * cut), bf16),
        jax.ShapeDtypeStruct((group, heads, rows), f32),
    )
    mixed, lse = pl.pallas_call(
        functools.partial(attend_kernel, n, n_tp, group, heads),
        out_shape=return_shapes,
        in_specs=[vmem] * 5,
        out_specs=(vmem, vmem),
        scratch_shapes=[
            VMEM((own, LANES), f32), VMEM((behind + own, LANES), f32), VMEM((behind + own, LANES), f32),
            VMEM((own, LANES), f32), VMEM((own, LANES), f32), VMEM((own, LANES), f32),
            VMEM((own, LANES), bf16), VMEM((group, heads, rows), f32),
            VMEM((n * cut, width), bf16), VMEM((group, rows, LANES), bf16),
            VMEM((n_tp, chunks, part, chunk), bf16), VMEM((n_tp, chunks, part, chunk), bf16),
            dma((planes,)),
            dma((planes, group)), dma((planes, group)),
            dma((planes, group)), dma((planes, group)),
            dma((group,)), dma((group,)), dma((group,)), dma((group,)),
            dma((n_tp, chunks)), dma((n_tp, chunks)),
            dma((3,)), dma((group,)),
        ],
        compiler_params=pltpu.CompilerParams(collective_id=1, has_side_effects=True, vmem_limit_bytes=48 << 20),
        cost_estimate=pl.CostEstimate(flops=1 << 32, bytes_accessed=1 << 22, transcendentals=1 << 22),
        name="attend",
    )(q, kv, halo, o_far, o_plane)
    return mixed, lse.reshape(group * heads, rows)


def solution(mesh):
    placed = (P("sp", None), P("sp", "tp"), P("sp", "tp"), P("sp", "tp"), P("tp", "sp"))
    return jax.shard_map(
        functools.partial(shards, mesh.shape["sp"], mesh.shape["tp"]),
        mesh=mesh,
        in_specs=placed,
        out_specs=(P(("sp", "tp"), None), P("tp", "sp")),
        check_vma=False,
    )
```
